128 devices in a mesh: sp: 16 (over z, y), tp: 8 (over x, core).
Axes of the slice: x: 4, y: 4, z: 4, core: 2. Of those that a mesh axis runs over, the one named last changes fastest.
Arguments:
- queries: bfloat16 [16384, 1024], P('sp', 'tp'), may hold values from -6 to 6
- keys: bfloat16 [16384, 1024], P('sp', 'tp'), may hold values from -6 to 6
- values: bfloat16 [16384, 1024], P('sp', 'tp'), may hold values from -6 to 6
- cum_gates: float32 [16384, 16], P('sp', 'tp'), may hold values from -2050 to 0, as said below
- doc_ids: int32 [16384], P('sp'), may hold values from 0 to 1, never falling along the last dimension, each value on 1 to 12288 neighbouring positions
- residual: bfloat16 [16384, 2048], P('sp', 'tp'), may hold values from -100 to 100
- w_out: bfloat16 [1024, 2048], P('tp'), may hold values from -0.1875 to 0.1875
- norm_gain: bfloat16 [2048], P('tp'), may hold values from 0.099609375 to 1.8984375
- w_up: bfloat16 [2048, 8192], P('sp', 'tp'), may hold values from -0.125 to 0.125
- w_down: bfloat16 [8192, 2048], P('tp', 'sp'), may hold values from -0.0625 to 0.0625
Outputs:
- output: bfloat16 [16384, 2048], P('sp', 'tp')
The draws below stay inside these ranges and needn't reach their ends.
Inputs may be any that keep to these rules, and one draw needn't show every extreme that they name: `cum_gates`: along positions each head's values never rise. `doc_ids`: document numbers never fall along positions; a document holds 1 to three quarters of 16384 positions.
All inputs are finite; a program needn't handle non-finite values.
Results may differ from the reference program's by a relative error of at most 0.015.
Values may be sent and summed in bfloat16 or wider, within the bound.
No kernel may reach another device: no remote copies, remote signals or barrier semaphores. Data moves between devices by JAX's collectives and lax.ppermute only.
A program may use at most 128 MiB of HBM per device.

```python
import math
import jax
import jax.numpy as jnp
import numpy as np
from jax import lax

D = 2048
HEAD_COUNT = 16
HD = 64
FF = 8192
TOK_DEV = 1024
TOKEN_COUNT = 16384
N_TP = 8


def draw_queries(key, part):
    shape_all = (TOKEN_COUNT, HEAD_COUNT * HD)
    drawn = jnp.clip(jax.random.normal(jax.random.fold_in(key, 11), shape_all, jnp.float32), -6.0, 6.0)
    return drawn.astype(jnp.bfloat16)


def draw_keys(key, part):
    shape_all = (TOKEN_COUNT, HEAD_COUNT * HD)
    drawn = jnp.clip(jax.random.normal(jax.random.fold_in(key, 13), shape_all, jnp.float32), -6.0, 6.0)
    return drawn.astype(jnp.bfloat16)


def draw_values(key, part):
    block_count = TOKEN_COUNT // TOK_DEV
    cols_all = HEAD_COUNT * HD
    block_means = jnp.clip(jax.random.normal(jax.random.fold_in(key, 21), (block_count, 1, cols_all), jnp.float32), -2.0, 2.0)
    draw_noise = jnp.clip(jax.random.normal(jax.random.fold_in(key, 23), (block_count, TOK_DEV, cols_all), jnp.float32), -4.6, 4.6)
    mean_weight = 0.7
    drawn = jnp.clip(draw_noise + mean_weight * block_means, -6.0, 6.0)
    return drawn.reshape(TOKEN_COUNT, cols_all).astype(jnp.bfloat16)


def draw_cum_gates(key, part):
    head_rank = jax.random.permutation(jax.random.fold_in(key, 31), HEAD_COUNT)
    fast_count = HEAD_COUNT // 2
    pos_factor = jax.random.uniform(jax.random.fold_in(key, 33), (TOKEN_COUNT, HEAD_COUNT), jnp.float32, 0.3, 1.7)
    fast_heads = head_rank < fast_count
    fast_rate = jnp.exp(jax.random.uniform(jax.random.fold_in(key, 34), (HEAD_COUNT,), jnp.float32, jnp.log(1.0 / 100.0), jnp.log(1.0 / 30.0)))
    slow_rate = jnp.exp(jax.random.uniform(jax.random.fold_in(key, 35), (HEAD_COUNT,), jnp.float32, jnp.log(0.1), jnp.log(0.4))) / TOKEN_COUNT
    head_rate = jnp.where(fast_heads, fast_rate, slow_rate)
    block_factor = jnp.exp(jax.random.uniform(jax.random.fold_in(key, 36), (TOKEN_COUNT // TOK_DEV,), jnp.float32, jnp.log(0.5), jnp.log(2.0)))
    block_factor = jnp.repeat(block_factor, TOK_DEV)
    gate_logarithm = -head_rate[None, :] * block_factor[:, None] * pos_factor
    spike_positions = jax.random.randint(jax.random.fold_in(key, 37), (2, HEAD_COUNT), 0, TOKEN_COUNT)
    spike_penalty = jnp.log(jax.random.uniform(jax.random.fold_in(key, 38), (2, HEAD_COUNT), jnp.float32, 0.5, 0.8))
    spike_matches = jnp.arange(TOKEN_COUNT, dtype=jnp.int32)[:, None, None] == spike_positions[None]
    gate_logarithm = gate_logarithm + jnp.sum(jnp.where(spike_matches, spike_penalty[None], 0.0), axis=1)
    return jnp.cumsum(gate_logarithm, axis=0).astype(jnp.float32)


def draw_residual(key, part):
    col_frac = jnp.arange(D, dtype=jnp.float32) / D
    col_low, col_span, row_low, row_high = (0.3, 10.0, 0.6, 1.6)
    jitter = jax.random.uniform(jax.random.fold_in(key, 41), (D,), jnp.float32, 0.7, 1.3)
    col_scale = col_low * col_span ** col_frac * jitter
    row_scale = jnp.exp(jax.random.uniform(jax.random.fold_in(key, 42), (TOKEN_COUNT, 1), jnp.float32, jnp.log(row_low), jnp.log(row_high)))
    drawn = jnp.clip(jax.random.normal(jax.random.fold_in(key, 43), (TOKEN_COUNT, D), jnp.float32), -6.0, 6.0)
    return (drawn * col_scale[None, :] * row_scale).astype(jnp.bfloat16)


def shard_levels(stream_key, dims, split, smallest, top_value):
    gain, own = 1.0, jax.random.fold_in(stream_key, 6)
    for position, shards_of in split:
        draws = jnp.exp(jax.random.uniform(jax.random.fold_in(own, position), (shards_of,), jnp.float32, smallest / len(split), top_value / len(split)))
        gain = gain * jnp.repeat(draws, dims[position] // shards_of).reshape([-1 if axis == position else 1 for axis in range(len(dims))])
    return gain


def profile(number_of, total, bound, slope):
    portions = [(1 << 20) // math.isqrt(standing ** slope) + 1 for standing in range(2, number_of + 1)]
    spare, holding = total - bound - (number_of - 1), [1] * (number_of - 1)
    while spare > 0:
        movable = [i for i in range(number_of - 1) if holding[i] < bound]
        whole, left = sum([portions[i] for i in movable]), spare
        for i in movable:
            addition = min(bound - holding[i], max(1, left * portions[i] // whole), spare)
            holding[i] = holding[i] + addition
            spare = spare - addition
    return np.array([bound] + holding)


def uneven(stream_key, count, total, bound, lean):
    if count == 2:
        one = jax.random.randint(stream_key, (), max(1, total - bound), min(bound, total - 1) + 1)
        return jnp.stack([one, total - one])
    tallies = jnp.asarray(profile(count, total, bound, lean), jnp.int32)
    pairs = (count - 1) // 2
    giver, receiver = tallies[1:1 + 2 * pairs:2], tallies[2:2 + 2 * pairs:2]
    slack = jnp.minimum(giver - 1, bound - receiver)
    passed = jax.random.randint(jax.random.fold_in(stream_key, 1), (pairs,), 0, 1 << 20) % (slack + 1)
    tallies = tallies.at[1:1 + 2 * pairs:2].set(giver - passed).at[2:2 + 2 * pairs:2].set(receiver + passed)
    return tallies[jax.random.permutation(jax.random.fold_in(stream_key, 2), count)]


def scatter_about(stream_key, extent, scale, bound, shards=(), kind=jnp.bfloat16):
    result = scale * jax.random.normal(stream_key, extent, jnp.float32)
    if shards:
        result = result * shard_levels(stream_key, extent, shards, -0.22, 0.18)
    return jnp.clip(result, -bound, bound).astype(kind)


def setup_inputs(seed: int = 0) -> dict:
    streams_of = jax.random.split(jax.random.key(seed), 11)
    queries = draw_queries(jax.random.fold_in(streams_of[10], 71), 0)
    keys = draw_keys(jax.random.fold_in(streams_of[10], 71), 0)
    values = draw_values(jax.random.fold_in(streams_of[10], 71), 0)
    cum_gates = draw_cum_gates(jax.random.fold_in(streams_of[10], 71), 0)
    doc_ids = jnp.searchsorted(jnp.cumsum(uneven(streams_of[4], 2, TOKEN_COUNT, TOKEN_COUNT * 3 // 4, 0)), jnp.arange(TOKEN_COUNT), side="right").astype(jnp.int32)
    residual = draw_residual(jax.random.fold_in(streams_of[10], 71), 0)
    w_out = scatter_about(streams_of[6], (HEAD_COUNT * HD, D), (HEAD_COUNT * HD) ** -0.5, 0.1875, ((0, 8),))
    norm_gain = jnp.clip(1.0 + 0.18 * jax.random.normal(streams_of[7], (D,), jnp.float32), 0.099609375, 1.8984375).astype(jnp.bfloat16)
    w_up = scatter_about(streams_of[8], (D, FF), D ** -0.5, 0.125, ((0, 16), (1, 8)))
    w_down = scatter_about(streams_of[9], (FF, D), FF ** -0.5, 0.0625, ((0, 8), (1, 16)))
    return dict(queries=queries, keys=keys, values=values, cum_gates=cum_gates, doc_ids=doc_ids, residual=residual, w_out=w_out, norm_gain=norm_gain, w_up=w_up, w_down=w_down)


eps = 1e-06

def rounded_back(value):
    return lax.optimization_barrier(value.astype(jnp.bfloat16)).astype(jnp.float32)

def reference(queries, keys, values, cum_gates, doc_ids, residual, w_out, norm_gain, w_up, w_down):
    seq_total = queries.shape[0]
    head_cols = queries.shape[1]
    head_count = head_cols // HD
    q_block = math.gcd(seq_total, 128)
    score_scale = HD ** (-0.5)
    keys_wide = keys.astype(jnp.float32).reshape(seq_total, head_count, HD)
    values_wide = values.astype(jnp.float32).reshape(seq_total, head_count, HD)
    gates_t = jnp.transpose(cum_gates)
    key_pos = jnp.arange(seq_total, dtype=jnp.int32)

    def attend_block(block_index):
        row_start = (block_index * q_block).astype(jnp.int32)
        q_rows = lax.dynamic_slice_in_dim(queries, row_start, q_block, 0).astype(jnp.float32)
        q_rows = q_rows.reshape(q_block, head_count, HD)
        gate_rows = lax.dynamic_slice_in_dim(gates_t, row_start, q_block, 1)
        doc_rows = lax.dynamic_slice_in_dim(doc_ids, row_start, q_block, 0)
        q_pos = row_start + jnp.arange(q_block, dtype=jnp.int32)
        scores = jnp.einsum('qhd,khd->hqk', q_rows, keys_wide) * score_scale
        scores = scores + gate_rows[:, :, None] - gates_t[:, None, :]
        visible = ((key_pos[None, :] <= q_pos[:, None]) & (doc_ids[None, :] == doc_rows[:, None]))[None]
        row_top = lax.optimization_barrier(jnp.max(jnp.where(visible, scores, -jnp.inf), axis=-1))
        weights = jnp.where(visible, jnp.exp(scores - row_top[..., None]), 0.0)
        weight_sum = lax.optimization_barrier(jnp.sum(weights, axis=-1))
        rounded = rounded_back(weights)
        summed = jnp.einsum('hqk,khd->qhd', rounded, values_wide)
        attended = summed / jnp.transpose(weight_sum)[:, :, None]
        return attended.reshape(q_block, head_cols).astype(jnp.bfloat16)
    attended = lax.map(attend_block, jnp.arange(seq_total // q_block, dtype=jnp.int32))
    attended = attended.reshape(seq_total, head_cols)
    group_cols = head_cols // N_TP
    head_mixed = jnp.zeros((seq_total, D), jnp.float32)
    for group_index in range(N_TP):
        low_col = group_index * group_cols
        partial_term = jnp.dot(attended[:, low_col:low_col + group_cols], w_out[low_col:low_col + group_cols], preferred_element_type=jnp.float32)
        head_mixed = head_mixed + rounded_back(partial_term)
    middle = (residual.astype(jnp.float32) + head_mixed).astype(jnp.bfloat16)
    middle_wide = lax.optimization_barrier(middle).astype(jnp.float32)
    mean_square = lax.optimization_barrier(jnp.mean(middle_wide * middle_wide, axis=-1, keepdims=True))
    normed = (middle_wide * lax.rsqrt(mean_square + eps) * norm_gain.astype(jnp.float32)).astype(jnp.bfloat16)
    up_proj = jnp.dot(normed, w_up, preferred_element_type=jnp.float32)
    hidden = jnp.square(jax.nn.relu(up_proj)).astype(jnp.bfloat16)
    unit_cols = FF // N_TP
    feed = jnp.zeros((seq_total, D), jnp.float32)
    for group_index in range(N_TP):
        low_unit = group_index * unit_cols
        partial_term = jnp.dot(hidden[:, low_unit:low_unit + unit_cols], w_down[low_unit:low_unit + unit_cols], preferred_element_type=jnp.float32)
        feed = feed + rounded_back(partial_term)
    return (middle_wide + feed).astype(jnp.bfloat16)
```

```python
import functools

import jax
import jax.numpy as jnp
from jax import lax
from jax.experimental import pallas as pl
from jax.experimental.pallas import tpu as pltpu
from jax.sharding import Mesh, PartitionSpec as P

D = 2048
HD = 64
TOK = 1024
HALF = 512
KROWS = 256
VROWS = 256
GROWS = 32
KV_ROWS = KROWS + VROWS + GROWS
Q_ROWS = 256

eps = 1e-06
far_below = -1e30
lowest = -1e29
RING = (1, 3, 2)


DIMS = (((1,), (0,)), ((), ()))


def score(i, pq, kv, ke, qa, qb, s_ref):
    keys = jnp.concatenate([kv[i, 0:KROWS, :], ke[i]], axis=1)
    for j in range(2):
        for part, q_ref in enumerate((qa, qb)):
            s_ref[j, 256 * part : 256 * (part + 1), :] = lax.dot_general(
                keys, q_ref[pq, :, 256 * j : 256 * (j + 1)], DIMS, preferred_element_type=jnp.float32
            )


def hide(s_ref, ahead, k_zero, q_zero):
    for j in range(2):
        for part in range(2):
            row = lax.broadcasted_iota(jnp.int32, (256, 256), 0)
            lane = lax.broadcasted_iota(jnp.int32, (256, 256), 1)
            seen = (row - lane <= ahead + 256 * (j - part)) & (
                (row >= k_zero - 256 * part) | (lane < q_zero - 256 * j)
            )
            at = slice(256 * part, 256 * (part + 1))
            s_ref[j, at, :] = jnp.where(seen, s_ref[j, at, :], far_below)


def weigh(pq, s_ref, p_ref, m_ref, l_ref, shrink_ref):
    for j in range(2):
        cols = slice(256 * j, 256 * (j + 1))
        top = jnp.max(s_ref[j, 0:64, :].reshape(8, 8, 256), axis=0)
        for n in range(1, 8):
            top = jnp.maximum(top, jnp.max(s_ref[j, 64 * n : 64 * (n + 1), :].reshape(8, 8, 256), axis=0))
        m_old = m_ref[pq, :, cols]
        m_new = jnp.maximum(m_old, jnp.max(top, axis=0, keepdims=True))
        shrink = jnp.exp(m_old - m_new)
        m_ref[pq, :, cols] = m_new
        shrink_ref[:, cols] = shrink
        sums = jnp.zeros((8, 256), jnp.float32)
        for n in range(8):
            p = jnp.exp(s_ref[j, 64 * n : 64 * (n + 1), :] - m_new)
            sums = sums + jnp.sum(p.reshape(8, 8, 256), axis=0)
            p_ref[j, 64 * n : 64 * (n + 1), :] = p.astype(jnp.bfloat16)
        l_ref[pq, :, cols] = l_ref[pq, :, cols] * shrink + jnp.sum(sums, axis=0, keepdims=True)


def blend(i, pq, kv, p_ref, shrink_ref, acc_ref):
    values = jnp.concatenate([kv[i, KROWS + 64 * n : KROWS + 64 * (n + 1), :] for n in range(4)], axis=1)
    for j in range(2):
        cols = slice(256 * j, 256 * (j + 1))
        product = lax.dot_general(values, p_ref[j], DIMS, preferred_element_type=jnp.float32)
        acc_ref[pq, :, cols] = acc_ref[pq, :, cols] * shrink_ref[:, cols] + product


def attend_kernel(n_arr, first, last, sc, qt_ref, *rest):
    kv_in, rest = rest[:n_arr], rest[n_arr:]
    if first:
        state_in = ()
    else:
        state_in, rest = rest[:3], rest[3:]
    if last:
        out_ref, rest = rest[0], rest[1:]
    m_ref, l_ref, acc_ref, kv, ke, qa, qb, s_a, s_b, p_a, p_b, shrink_a, shrink_b, zero_s, todo, sems = rest
    copies = [
        pltpu.make_async_copy(kv_in[n], kv.at[pl.ds(4 * n, 4)], sems.at[n]) for n in range(n_arr)
    ]
    for copy in copies:
        copy.start()
    if first:
        m_ref[...] = jnp.full(m_ref.shape, lowest, jnp.float32)
        l_ref[...] = jnp.zeros(l_ref.shape, jnp.float32)
        acc_ref[...] = jnp.zeros(acc_ref.shape, jnp.float32)
    else:
        m_ref[...] = state_in[0][...]
        l_ref[...] = state_in[1][...]
        acc_ref[...] = state_in[2][...]
    row = lax.broadcasted_iota(jnp.int32, (128, HALF), 0)
    minus_a = jnp.where(row < 3, -1.0, 0.0).astype(jnp.bfloat16)
    minus_b = jnp.where((row >= 3) & (row < 6), -1.0, 0.0).astype(jnp.bfloat16)
    zeros = jnp.zeros((64, HALF), jnp.bfloat16)
    for pq in range(4):
        q = jnp.concatenate([qt_ref[pq, 64 * n : 64 * (n + 1), :] for n in range(4)], axis=1)
        qa[pq, 0:64, :] = q
        qa[pq, 64:128, :] = zeros
        qa[pq, 128:256, :] = minus_a
        qb[pq, 0:64, :] = zeros
        qb[pq, 64:128, :] = q
        qb[pq, 128:256, :] = minus_b
    for copy in copies:
        copy.wait()
    blank = jnp.zeros((112, 128), jnp.float32)

    def prepare(n, carry):
        for k in range(4):
            i = 4 * n + k
            g = kv[i, KROWS + VROWS : KV_ROWS, :].astype(jnp.float32)
            for half in range(2):
                turned = jnp.concatenate([g[16 * half : 16 * (half + 1)], blank], axis=0).T
                ke[i, 128 * half : 128 * (half + 1), :] = turned.astype(jnp.bfloat16)
            zero_s[i] = HALF - jnp.sum(g[8:16]).astype(jnp.int32)
        return carry

    lax.fori_loop(0, n_arr, prepare, 0)

    def list_keys(i, count):
        arr = i // 4
        k_start = ((i % 4) ^ sc[7 + 2 * arr]) * 4096 + sc[6 + 2 * arr]
        k_zero = zero_s[i]
        for pq in range(4):
            ahead = (pq ^ sc[1]) * 4096 + sc[0] - k_start
            q_zero = sc[2 + pq]
            live = (ahead > -HALF) & jnp.logical_not((k_zero == HALF) & (q_zero == 0))
            full = (ahead >= HALF) & ((k_zero == 0) | (q_zero == HALF))
            todo[count, 0] = i
            todo[count, 1] = pq
            todo[count, 2] = ahead
            todo[count, 3] = jnp.where(full, 0, 1)
            count = count + live.astype(jnp.int32)
        return count

    count = lax.fori_loop(0, 4 * n_arr, list_keys, 0)
    for extra in range(2):
        todo[count + extra, 0] = 0
        todo[count + extra, 1] = 0
        todo[count + extra, 2] = -100000
        todo[count + extra, 3] = 1

    p_b[...] = jnp.zeros(p_b.shape, jnp.bfloat16)
    shrink_b[...] = jnp.ones(shrink_b.shape, jnp.float32)
    score(todo[0, 0], todo[0, 1], kv, ke, qa, qb, s_a)

    def step(t, now, later):
        s_now, p_now, shrink_now = now
        s_later, p_later, shrink_later = later
        before = jnp.maximum(t - 1, 0)

        @pl.when(todo[t, 3] == 1)
        def _():
            hide(s_now, todo[t, 2], zero_s[todo[t, 0]], sc[2 + todo[t, 1]])

        score(todo[t + 1, 0], todo[t + 1, 1], kv, ke, qa, qb, s_later)
        weigh(todo[t, 1], s_now, p_now, m_ref, l_ref, shrink_now)
        blend(todo[before, 0], todo[before, 1], kv, p_later, shrink_later, acc_ref)

    def two_steps(n, carry):
        side_a, side_b = (s_a, p_a, shrink_a), (s_b, p_b, shrink_b)
        step(2 * n, side_a, side_b)
        step(2 * n + 1, side_b, side_a)
        return carry

    rounds = (count + 1) // 2
    lax.fori_loop(0, rounds, two_steps, 0)

    @pl.when(rounds > 0)
    def _():
        at = 2 * rounds - 1
        blend(todo[at, 0], todo[at, 1], kv, p_b, shrink_b, acc_ref)

    if last:

        def finish(pq, carry):
            out = (acc_ref[pq] / l_ref[pq]).astype(jnp.bfloat16)
            block = pq ^ sc[1]
            for quarter in range(4):
                out_ref[quarter * 4 + block] = out[:, 128 * quarter : 128 * (quarter + 1)]
            return carry

        lax.fori_loop(0, 4, finish, 0)


def attend(scalars, qt, arrays, state, first, last):
    n_arr = len(arrays)
    vmem = pl.BlockSpec(memory_space=pltpu.VMEM)
    shapes = [
        jax.ShapeDtypeStruct((4, 1, HALF), jnp.float32),
        jax.ShapeDtypeStruct((4, 1, HALF), jnp.float32),
        jax.ShapeDtypeStruct((4, HD, HALF), jnp.float32),
    ]
    scratch = [
        pltpu.VMEM((4 * n_arr, KV_ROWS, 128), jnp.bfloat16),
        pltpu.VMEM((4 * n_arr, 256, 128), jnp.bfloat16),
        pltpu.VMEM((4, 256, HALF), jnp.bfloat16),
        pltpu.VMEM((4, 256, HALF), jnp.bfloat16),
        pltpu.VMEM((2, HALF, 256), jnp.float32),
        pltpu.VMEM((2, HALF, 256), jnp.float32),
        pltpu.VMEM((2, HALF, 256), jnp.bfloat16),
        pltpu.VMEM((2, HALF, 256), jnp.bfloat16),
        pltpu.VMEM((1, HALF), jnp.float32),
        pltpu.VMEM((1, HALF), jnp.float32),
        pltpu.SMEM((4 * n_arr,), jnp.int32),
        pltpu.SMEM((16 * n_arr + 2, 4), jnp.int32),
        pltpu.SemaphoreType.DMA((n_arr,)),
    ]
    if last:
        out_shape = jax.ShapeDtypeStruct((16, HD, 128), jnp.bfloat16)
        out_specs = vmem
        scratch = [pltpu.VMEM(s.shape, s.dtype) for s in shapes] + scratch
    else:
        out_shape = shapes
        out_specs = [vmem] * 3
    state = () if first else tuple(state)
    return pl.pallas_call(
        functools.partial(attend_kernel, n_arr, first, last),
        out_shape=out_shape,
        in_specs=[pl.BlockSpec(memory_space=pltpu.SMEM), vmem]
        + [pl.BlockSpec(memory_space=pl.ANY)] * n_arr
        + [vmem] * len(state),
        out_specs=out_specs,
        scratch_shapes=scratch,
        compiler_params=pltpu.CompilerParams(vmem_limit_bytes=40 * 1024 * 1024),
        cost_estimate=pl.CostEstimate(
            flops=4_000_000_000 * n_arr, bytes_accessed=1_000_000 * n_arr, transcendentals=0
        ),
        name="attend_first" if first else ("attend_last" if last else "attend_more"),
    )(scalars, qt, *arrays, *state)


def dense_kernel(sc, att_ref, res_ref, *rest):
    w_in, (mid_ref, gain_ref, w_all, sems) = rest[:8], rest[8:]
    copies = []
    for n in range(8):
        at = pl.multiple_of(sc[n], 128)
        lanes = pl.ds(pl.multiple_of(sc[n] * 2, 256), 256)
        copies.append(pltpu.make_async_copy(w_in[n].at[pl.ds(0, 128)], w_all.at[pl.ds(at, 128)], sems.at[n]))
        copies.append(
            pltpu.make_async_copy(w_in[n].at[pl.ds(128, 8), pl.ds(0, 256)], gain_ref.at[:, lanes], sems.at[8 + n])
        )
    for copy in copies:
        copy.start()
    for copy in copies:
        copy.wait()
    att = att_ref[...].reshape(1024, 128)
    for n in range(8):
        tp = 2 * (n % 4) + n // 4
        cols = slice(256 * tp, 256 * (tp + 1))
        mixed = lax.dot_general(
            att, w_all[:, cols], (((0,), (0,)), ((), ())), preferred_element_type=jnp.float32
        )
        mid_ref[:, cols] = (res_ref[n].astype(jnp.float32) + mixed).astype(jnp.bfloat16)


def dense(scalars, att, res, pieces):
    vmem = pl.BlockSpec(memory_space=pltpu.VMEM)
    return pl.pallas_call(
        dense_kernel,
        out_shape=[
            jax.ShapeDtypeStruct((128, D), jnp.bfloat16),
            jax.ShapeDtypeStruct((8, D), jnp.bfloat16),
        ],
        in_specs=[pl.BlockSpec(memory_space=pltpu.SMEM), vmem, vmem] + [pl.BlockSpec(memory_space=pl.ANY)] * 8,
        out_specs=[vmem, vmem],
        scratch_shapes=[pltpu.VMEM((1024, D), jnp.bfloat16), pltpu.SemaphoreType.DMA((16,))],
        compiler_params=pltpu.CompilerParams(vmem_limit_bytes=24 * 1024 * 1024),
        cost_estimate=pl.CostEstimate(flops=1_000_000_000, bytes_accessed=4_000_000, transcendentals=0),
        name="dense",
    )(scalars, att, res, *pieces)


def up_kernel(sc, gain_ref, w_in, *rest):
    mids, (h_ref, own_ref, w_up, mid_all, sems) = rest[:8], rest[8:]
    fetches = [pltpu.make_async_copy(mids[n], mid_all.at[pl.ds(128 * n, 128)], sems.at[16 + n]) for n in range(8)]
    copies = [
        pltpu.make_async_copy(w_in.at[pl.ds(256 * n, 128)], w_up.at[pl.ds(128 * n, 128)], sems.at[n]) for n in range(16)
    ]
    for copy in copies + fetches:
        copy.start()
    gain = gain_ref[0:1, :].astype(jnp.float32)
    for copy in copies:
        copy.wait()
    lanes = pl.ds(pl.multiple_of(sc[8], 256), 256)
    for n in range(0, 8, 2):
        for k in range(2):
            fetches[n + k].wait()
            own_ref[pl.ds(pl.multiple_of(sc[n + k], 128), 128), :] = mid_all[128 * (n + k) : 128 * (n + k + 1), lanes]
        wide = mid_all[128 * n : 128 * (n + 2), :].astype(jnp.float32)
        scale = lax.rsqrt(jnp.sum(wide * wide, axis=-1, keepdims=True) / D + eps)
        normed = (wide * scale * gain).astype(jnp.bfloat16)
        h = jnp.dot(normed, w_up[...], preferred_element_type=jnp.float32)
        h = jnp.square(jnp.maximum(h, 0.0)).astype(jnp.bfloat16)
        for k in range(2):
            h_ref[pl.ds(pl.multiple_of(sc[n + k], 128), 128), :] = h[128 * k : 128 * (k + 1)]


def up(scalars, gain, w, mids):
    vmem = pl.BlockSpec(memory_space=pltpu.VMEM)
    return pl.pallas_call(
        up_kernel,
        out_shape=[
            jax.ShapeDtypeStruct((1024, 1024), jnp.bfloat16),
            jax.ShapeDtypeStruct((1024, 256), jnp.bfloat16),
        ],
        in_specs=[pl.BlockSpec(memory_space=pltpu.SMEM), vmem] + [pl.BlockSpec(memory_space=pl.ANY)] * 9,
        out_specs=[vmem, vmem],
        scratch_shapes=[
            pltpu.VMEM((D, 1024), jnp.bfloat16),
            pltpu.VMEM((1024, D), jnp.bfloat16),
            pltpu.SemaphoreType.DMA((24,)),
        ],
        compiler_params=pltpu.CompilerParams(vmem_limit_bytes=40 * 1024 * 1024),
        cost_estimate=pl.CostEstimate(flops=4_300_000_000, bytes_accessed=8_000_000, transcendentals=0),
        name="up",
    )(scalars, gain, w, *mids)


def down_kernel(sc, h_ref, w_in, mine_ref, other_ref, w_down, sems):
    copies = []
    for k in range(4):
        at = pl.multiple_of((sc[0] + k) * 256 + 128, 128)
        copies.append(pltpu.make_async_copy(w_in.at[pl.ds(at, 128)], w_down.at[pl.ds(128 * k, 128)], sems.at[k]))
    for copy in copies:
        copy.start()
    for copy in copies:
        copy.wait()
    for n, out_ref in ((1 - sc[1], other_ref), (sc[1], mine_ref)):
        rows = w_down[pl.ds(pl.multiple_of(n * 256, 256), 256), :]
        product = lax.dot_general(
            h_ref[...], rows, (((1,), (1,)), ((), ())), preferred_element_type=jnp.float32
        )
        out_ref[...] = product.astype(out_ref.dtype)


def down(scalars, h, w):
    vmem = pl.BlockSpec(memory_space=pltpu.VMEM)
    return pl.pallas_call(
        down_kernel,
        out_shape=[
            jax.ShapeDtypeStruct((1024, 256), jnp.bfloat16),
            jax.ShapeDtypeStruct((1024, 256), jnp.bfloat16),
        ],
        in_specs=[pl.BlockSpec(memory_space=pltpu.SMEM), vmem, pl.BlockSpec(memory_space=pl.ANY)],
        out_specs=[vmem, vmem],
        scratch_shapes=[pltpu.VMEM((512, 1024), jnp.bfloat16), pltpu.SemaphoreType.DMA((4,))],
        compiler_params=pltpu.CompilerParams(vmem_limit_bytes=24 * 1024 * 1024),
        cost_estimate=pl.CostEstimate(flops=1_100_000_000, bytes_accessed=4_000_000, transcendentals=0),
        name="down",
    )(scalars, h, w)


def shifted(value, axis, by):
    n = lax.axis_size(axis)
    return lax.ppermute(value, axis, [(i, (i - by) % n) for i in range(n)])


def partner(value):
    return lax.ppermute(value, "c", [(0, 1), (1, 0)])


def body(queries, keys, values, cum_gates, doc_ids, residual, w_out, norm_gain, w_up, w_down):
    z, y, x, c = (lax.axis_index(a) for a in ("z", "y", "x", "c"))

    q_t = jnp.transpose(queries * jnp.bfloat16(0.125)).reshape(2, HD, 2, 4, 128)
    q_msg = jnp.transpose(q_t, (0, 2, 3, 1, 4)).reshape(2, 2, Q_ROWS, 128)
    v_t = jnp.transpose(values).reshape(2, HD, 2, 4, 128)
    v_msg = jnp.transpose(v_t, (0, 2, 3, 1, 4)).reshape(2, 2, VROWS, 128)
    k_msg = jnp.transpose(keys.reshape(2, 2, KROWS, 2, HD), (3, 0, 2, 1, 4)).reshape(2, 2, KROWS, 128)
    gates = jnp.transpose(cum_gates).reshape(2, 2, 2, 2, 128)
    hi = lax.reduce_precision(gates, 8, 7)
    mid = lax.reduce_precision(gates - hi, 8, 7)
    low = gates - hi - mid
    three = jnp.transpose(jnp.stack([hi, mid, low]), (1, 2, 4, 3, 0, 5)).reshape(2, 2, 2, 6, 128)
    docs = jnp.broadcast_to(doc_ids.astype(jnp.float32).reshape(1, 2, 4, 128), (2, 2, 4, 128))
    docs = jnp.stack([docs, jnp.zeros_like(docs)], axis=2)
    three = jnp.pad(three, ((0, 0), (0, 0), (0, 0), (0, 2), (0, 0)))
    docs = jnp.pad(docs, ((0, 0), (0, 0), (0, 0), (0, 4), (0, 0)))
    g_msg = jnp.concatenate([three, docs], axis=3).reshape(2, 2, GROWS, 128).astype(jnp.bfloat16)
    messages = jnp.concatenate([k_msg, v_msg, g_msg, q_msg], axis=2)

    received = []
    for step in range(4):
        pairs = []
        for zs in range(4):
            for cs in range(2):
                j = 2 * cs + ((zs & 1) ^ (step & 1))
                cd = (zs >> 1) ^ (step >> 1)
                pairs.append((zs * 2 + cs, j * 2 + cd))
        head = (z & 1) ^ (step & 1)
        half = (z >> 1) ^ (step >> 1)
        message = lax.dynamic_slice(messages, (head, half, 0, 0), (1, 1, KV_ROWS + Q_ROWS, 128))[0, 0]
        received.append(lax.ppermute(message, ("z", "c"), pairs))
    qt = jnp.stack([r[KV_ROWS:] for r in received])
    kv_own = jnp.stack([r[:KV_ROWS] for r in received])

    kv_mine = [kv_own] + [shifted(kv_own, "y", r) for r in RING]

    kv_own, w_out, residual, norm_gain, w_up, w_down = lax.optimization_barrier(
        (kv_own, w_out, residual, norm_gain, w_up, w_down)
    )
    both = jnp.concatenate([w_up, jnp.transpose(w_down)], axis=0)

    q_zero = HALF - jnp.sum(kv_own[:, KROWS + VROWS + 8 : KROWS + VROWS + 16].astype(jnp.float32), axis=(1, 2))
    mask_a = (z & 1) | (c << 1)
    mask_b = (z & 1) | ((1 - c) << 1)
    base = [y * TOK + c * HALF, mask_a] + [q_zero[n].astype(jnp.int32) for n in range(4)]

    def places(rs):
        out = []
        for r in rs:
            at = ((y + r) % 4) * TOK
            out += [at + c * HALF, mask_a, at + (1 - c) * HALF, mask_b]
        return jnp.stack(base + out).astype(jnp.int32)

    kv_near = partner(kv_own)
    state = attend(places([0]), qt, [kv_own, kv_near], (), True, False)
    gain_row = jnp.pad(norm_gain[None], ((0, 7), (0, D - 256)))
    w_msg = jnp.concatenate([w_out, gain_row], axis=0)
    w_mine = [w_msg] + [shifted(w_msg, "x", r) for r in RING]
    res = lax.all_to_all(residual.reshape(8, 128, 256), ("c", "x"), 0, 0, tiled=True)
    kv_mine[1:], state, both = lax.optimization_barrier((kv_mine[1:], state, both))
    both = lax.all_gather(both, ("z", "y"), axis=0, tiled=True)
    kv_other = [None] + [partner(piece) for piece in kv_mine[1:]]
    pieces = [piece for pair in zip(kv_mine[1:], kv_other[1:]) for piece in pair]
    out = attend(places(RING), qt, pieces, state, False, True)

    w_mine, res, out = lax.optimization_barrier((w_mine, res, out))
    w_pieces = [w for mine in w_mine for w in (mine, partner(mine))]

    attended = lax.all_to_all(out, ("x", "z"), 0, 0, tiled=True)

    order = [((x + r) % 4, cs) for r in (0, 1, 3, 2) for cs in (c, 1 - c)]
    rows_at = jnp.stack([xs * 256 + cs * 128 for xs, cs in order]).astype(jnp.int32)
    middle, gain = dense(rows_at, attended, res, w_pieces)

    mid_mine = [middle] + [shifted(middle, "x", r) for r in RING]
    mids = [m for mine in mid_mine for m in (mine, partner(mine))]
    token_at = jnp.stack([cs * 512 + xs * 128 for xs, cs in order] + [(2 * x + c) * 256]).astype(jnp.int32)
    hidden, middle_own = up(token_at, gain, both, mids)

    total = middle_own.astype(jnp.float32)
    for r in (2, 1, 3, 0):
        mine, other = down(jnp.stack([((x + r) % 4) * 4, c]).astype(jnp.int32), hidden, both)
        chip = mine.astype(jnp.float32) + partner(other).astype(jnp.float32)
        if r:
            chip = shifted(chip.astype(jnp.bfloat16), "x", -r).astype(jnp.float32)
        total = total + chip
    return total.astype(jnp.bfloat16)


def solution(mesh):
    split = Mesh(mesh.devices.reshape(4, 4, 4, 2), ("z", "y", "x", "c"))
    sp, tp = ("z", "y"), ("x", "c")
    in_specs = (
        P(sp, tp),
        P(sp, tp),
        P(sp, tp),
        P(sp, tp),
        P(sp),
        P(sp, tp),
        P(tp, None),
        P(tp),
        P(sp, tp),
        P(tp, sp),
    )
    return jax.shard_map(body, mesh=split, in_specs=in_specs, out_specs=P(sp, tp), check_vma=False)
```

```python
import functools

import jax
import jax.numpy as jnp
import numpy as np
from jax import lax
from jax.experimental import pallas as pl
from jax.experimental.pallas import tpu as pltpu
from jax.sharding import Mesh, PartitionSpec as P

D = 2048
HD = 64
TOK = 1024
HALF = 512
KROWS = 256
VROWS = 256
GROWS = 32
KV_ROWS = KROWS + VROWS + GROWS
Q_ROWS = 256

eps = 1e-06
far_below = -1e30
lowest = -1e29
RING = (1, 3, 2)


def in_hbm(arrays):
    return [pltpu.with_memory_space_constraint(a, pltpu.HBM) for a in arrays]


DIMS = (((1,), (0,)), ((), ()))


def score(i, pq, kv, ke, qa, qb, s_ref):
    keys = jnp.concatenate([kv[i, 0:KROWS, :], ke[i]], axis=1)
    for j in range(2):
        for part, q_ref in enumerate((qa, qb)):
            s_ref[j, 256 * part : 256 * (part + 1), :] = lax.dot_general(
                keys, q_ref[pq, :, 256 * j : 256 * (j + 1)], DIMS, preferred_element_type=jnp.float32
            )


def hide(s_ref, ahead, k_zero, q_zero):
    for j in range(2):
        for part in range(2):
            row = lax.broadcasted_iota(jnp.int32, (256, 256), 0)
            lane = lax.broadcasted_iota(jnp.int32, (256, 256), 1)
            seen = (row - lane <= ahead + 256 * (j - part)) & (
                (row >= k_zero - 256 * part) | (lane < q_zero - 256 * j)
            )
            at = slice(256 * part, 256 * (part + 1))
            s_ref[j, at, :] = jnp.where(seen, s_ref[j, at, :], far_below)


def weigh(pq, s_ref, p_ref, m_ref, l_ref, shrink_ref):
    for j in range(2):
        cols = slice(256 * j, 256 * (j + 1))
        top = jnp.max(s_ref[j, 0:64, :].reshape(8, 8, 256), axis=0)
        for n in range(1, 8):
            top = jnp.maximum(top, jnp.max(s_ref[j, 64 * n : 64 * (n + 1), :].reshape(8, 8, 256), axis=0))
        m_old = m_ref[pq, :, cols]
        m_new = jnp.maximum(m_old, jnp.max(top, axis=0, keepdims=True))
        shrink = jnp.exp(m_old - m_new)
        m_ref[pq, :, cols] = m_new
        shrink_ref[:, cols] = shrink
        sums = jnp.zeros((8, 256), jnp.float32)
        for n in range(8):
            p = jnp.exp(s_ref[j, 64 * n : 64 * (n + 1), :] - m_new)
            sums = sums + jnp.sum(p.reshape(8, 8, 256), axis=0)
            p_ref[j, 64 * n : 64 * (n + 1), :] = p.astype(jnp.bfloat16)
        l_ref[pq, :, cols] = l_ref[pq, :, cols] * shrink + jnp.sum(sums, axis=0, keepdims=True)


def blend(i, pq, kv, p_ref, shrink_ref, acc_ref):
    values = jnp.concatenate([kv[i, KROWS + 64 * n : KROWS + 64 * (n + 1), :] for n in range(4)], axis=1)
    for j in range(2):
        cols = slice(256 * j, 256 * (j + 1))
        product = lax.dot_general(values, p_ref[j], DIMS, preferred_element_type=jnp.float32)
        acc_ref[pq, :, cols] = acc_ref[pq, :, cols] * shrink_ref[:, cols] + product


def attend_kernel(n_arr, first, last, tab, zeros_q, qt_ref, *rest):
    kv_in, rest = rest[:n_arr], rest[n_arr:]
    if first:
        state_in = ()
    else:
        state_in, rest = rest[:3], rest[3:]
    if last:
        out_ref, rest = rest[0], rest[1:]
    m_ref, l_ref, acc_ref, kv, ke, qa, qb, s_a, s_b, p_a, p_b, shrink_a, shrink_b, zero_s, todo, sems = rest
    at_keys = 2 if first else 6
    copies = [
        pltpu.make_async_copy(kv_in[n], kv.at[pl.ds(4 * n, 4)], sems.at[n]) for n in range(n_arr)
    ]
    for copy in copies:
        copy.start()
    if first:
        m_ref[...] = jnp.full(m_ref.shape, lowest, jnp.float32)
        l_ref[...] = jnp.zeros(l_ref.shape, jnp.float32)
        acc_ref[...] = jnp.zeros(acc_ref.shape, jnp.float32)
    else:
        m_ref[...] = state_in[0][...]
        l_ref[...] = state_in[1][...]
        acc_ref[...] = state_in[2][...]
    row = lax.broadcasted_iota(jnp.int32, (128, HALF), 0)
    minus_a = jnp.where(row < 3, -1.0, 0.0).astype(jnp.bfloat16)
    minus_b = jnp.where((row >= 3) & (row < 6), -1.0, 0.0).astype(jnp.bfloat16)
    zeros = jnp.zeros((64, HALF), jnp.bfloat16)
    for pq in range(4):
        q = jnp.concatenate([qt_ref[pq, 64 * n : 64 * (n + 1), :] for n in range(4)], axis=1)
        qa[pq, 0:64, :] = q
        qa[pq, 64:128, :] = zeros
        qa[pq, 128:256, :] = minus_a
        qb[pq, 0:64, :] = zeros
        qb[pq, 64:128, :] = q
        qb[pq, 128:256, :] = minus_b
    for copy in copies:
        copy.wait()
    blank = jnp.zeros((112, 128), jnp.float32)

    def prepare(n, carry):
        for k in range(4):
            i = 4 * n + k
            g = kv[i, KROWS + VROWS : KV_ROWS, :].astype(jnp.float32)
            for half in range(2):
                turned = jnp.concatenate([g[16 * half : 16 * (half + 1)], blank], axis=0).T
                ke[i, 128 * half : 128 * (half + 1), :] = turned.astype(jnp.bfloat16)
            zero_s[i] = HALF - jnp.sum(g[8:16]).astype(jnp.int32)
        return carry

    lax.fori_loop(0, n_arr, prepare, 0)

    def list_keys(i, count):
        arr = i // 4
        k_start = ((i % 4) ^ tab[at_keys + 1 + 2 * arr]) * 4096 + tab[at_keys + 2 * arr]
        k_zero = zero_s[i]
        for pq in range(4):
            ahead = (pq ^ tab[1]) * 4096 + tab[0] - k_start
            q_zero = zeros_q[pq]
            live = (ahead > -HALF) & jnp.logical_not((k_zero == HALF) & (q_zero == 0))
            full = (ahead >= HALF) & ((k_zero == 0) | (q_zero == HALF))
            todo[count, 0] = i
            todo[count, 1] = pq
            todo[count, 2] = ahead
            todo[count, 3] = jnp.where(full, 0, 1)
            count = count + live.astype(jnp.int32)
        return count

    count = lax.fori_loop(0, 4 * n_arr, list_keys, 0)
    for extra in range(2):
        todo[count + extra, 0] = 0
        todo[count + extra, 1] = 0
        todo[count + extra, 2] = -100000
        todo[count + extra, 3] = 1

    p_b[...] = jnp.zeros(p_b.shape, jnp.bfloat16)
    shrink_b[...] = jnp.ones(shrink_b.shape, jnp.float32)
    score(todo[0, 0], todo[0, 1], kv, ke, qa, qb, s_a)

    def step(t, now, later):
        s_now, p_now, shrink_now = now
        s_later, p_later, shrink_later = later
        before = jnp.maximum(t - 1, 0)

        @pl.when(todo[t, 3] == 1)
        def _():
            hide(s_now, todo[t, 2], zero_s[todo[t, 0]], zeros_q[todo[t, 1]])

        score(todo[t + 1, 0], todo[t + 1, 1], kv, ke, qa, qb, s_later)
        weigh(todo[t, 1], s_now, p_now, m_ref, l_ref, shrink_now)
        blend(todo[before, 0], todo[before, 1], kv, p_later, shrink_later, acc_ref)

    def two_steps(n, carry):
        side_a, side_b = (s_a, p_a, shrink_a), (s_b, p_b, shrink_b)
        step(2 * n, side_a, side_b)
        step(2 * n + 1, side_b, side_a)
        return carry

    rounds = (count + 1) // 2
    lax.fori_loop(0, rounds, two_steps, 0)

    @pl.when(rounds > 0)
    def _():
        at = 2 * rounds - 1
        blend(todo[at, 0], todo[at, 1], kv, p_b, shrink_b, acc_ref)

    if last:

        def finish(pq, carry):
            out = (acc_ref[pq] / l_ref[pq]).astype(jnp.bfloat16)
            block = pq ^ tab[1]
            for quarter in range(4):
                out_ref[quarter * 4 + block] = out[:, 128 * quarter : 128 * (quarter + 1)]
            return carry

        lax.fori_loop(0, 4, finish, 0)


def attend(table, zeros_q, qt, arrays, state, first, last):
    n_arr = len(arrays)
    vmem = pl.BlockSpec(memory_space=pltpu.VMEM)
    shapes = [
        jax.ShapeDtypeStruct((4, 1, HALF), jnp.float32),
        jax.ShapeDtypeStruct((4, 1, HALF), jnp.float32),
        jax.ShapeDtypeStruct((4, HD, HALF), jnp.float32),
    ]
    scratch = [
        pltpu.VMEM((4 * n_arr, KV_ROWS, 128), jnp.bfloat16),
        pltpu.VMEM((4 * n_arr, 256, 128), jnp.bfloat16),
        pltpu.VMEM((4, 256, HALF), jnp.bfloat16),
        pltpu.VMEM((4, 256, HALF), jnp.bfloat16),
        pltpu.VMEM((2, HALF, 256), jnp.float32),
        pltpu.VMEM((2, HALF, 256), jnp.float32),
        pltpu.VMEM((2, HALF, 256), jnp.bfloat16),
        pltpu.VMEM((2, HALF, 256), jnp.bfloat16),
        pltpu.VMEM((1, HALF), jnp.float32),
        pltpu.VMEM((1, HALF), jnp.float32),
        pltpu.SMEM((4 * n_arr,), jnp.int32),
        pltpu.SMEM((16 * n_arr + 2, 4), jnp.int32),
        pltpu.SemaphoreType.DMA((n_arr,)),
    ]
    if last:
        out_shape = jax.ShapeDtypeStruct((16, HD, 128), jnp.bfloat16)
        out_specs = vmem
        scratch = [pltpu.VMEM(s.shape, s.dtype) for s in shapes] + scratch
    else:
        out_shape = shapes
        out_specs = [vmem] * 3
    state = () if first else tuple(state)
    return pl.pallas_call(
        functools.partial(attend_kernel, n_arr, first, last),
        out_shape=out_shape,
        in_specs=[pl.BlockSpec(memory_space=pltpu.SMEM)] * 2
        + [vmem]
        + [pl.BlockSpec(memory_space=pltpu.HBM)] * n_arr
        + [vmem] * len(state),
        out_specs=out_specs,
        scratch_shapes=scratch,
        compiler_params=pltpu.CompilerParams(vmem_limit_bytes=40 * 1024 * 1024),
        cost_estimate=pl.CostEstimate(
            flops=4_000_000_000 * n_arr, bytes_accessed=1_000_000 * n_arr, transcendentals=0
        ),
        name="attend_first" if first else ("attend_last" if last else "attend_more"),
    )(table, zeros_q, qt, *in_hbm(arrays), *state)


def dense_kernel(sc, att_ref, res_ref, *rest):
    w_in, (mid_ref, gain_ref, w_all, sems) = rest[:8], rest[8:]
    copies = []
    for n in range(8):
        at = pl.multiple_of(sc[18 + n], 128)
        lanes = pl.ds(pl.multiple_of(sc[18 + n] * 2, 256), 256)
        copies.append(pltpu.make_async_copy(w_in[n].at[pl.ds(0, 128)], w_all.at[pl.ds(at, 128)], sems.at[n]))
        copies.append(
            pltpu.make_async_copy(w_in[n].at[pl.ds(128, 8), pl.ds(0, 256)], gain_ref.at[:, lanes], sems.at[8 + n])
        )
    for copy in copies:
        copy.start()
    for copy in copies:
        copy.wait()
    att = att_ref[...].reshape(1024, 128)
    for n in range(8):
        tp = 2 * (n % 4) + n // 4
        cols = slice(256 * tp, 256 * (tp + 1))
        mixed = lax.dot_general(
            att, w_all[:, cols], (((0,), (0,)), ((), ())), preferred_element_type=jnp.float32
        )
        mid_ref[:, cols] = (res_ref[n].astype(jnp.float32) + mixed).astype(jnp.bfloat16)


def dense(scalars, att, res, pieces):
    vmem = pl.BlockSpec(memory_space=pltpu.VMEM)
    return pl.pallas_call(
        dense_kernel,
        out_shape=[
            jax.ShapeDtypeStruct((128, D), jnp.bfloat16),
            jax.ShapeDtypeStruct((8, D), jnp.bfloat16),
        ],
        in_specs=[pl.BlockSpec(memory_space=pltpu.SMEM), vmem, vmem] + [pl.BlockSpec(memory_space=pltpu.HBM)] * 8,
        out_specs=[vmem, vmem],
        scratch_shapes=[pltpu.VMEM((1024, D), jnp.bfloat16), pltpu.SemaphoreType.DMA((16,))],
        compiler_params=pltpu.CompilerParams(vmem_limit_bytes=24 * 1024 * 1024),
        cost_estimate=pl.CostEstimate(flops=1_000_000_000, bytes_accessed=4_000_000, transcendentals=0),
        name="dense",
    )(scalars, att, res, *in_hbm(pieces))


def up_kernel(sc, gain_ref, w_in, *rest):
    mids, (h_ref, own_ref, w_up, mid_all, normed, sems) = rest[:8], rest[8:]
    fetches = [pltpu.make_async_copy(mids[n], mid_all.at[pl.ds(128 * n, 128)], sems.at[16 + n]) for n in range(8)]
    copies = [
        pltpu.make_async_copy(w_in.at[pl.ds(256 * n, 128)], w_up.at[pl.ds(128 * n, 128)], sems.at[n]) for n in range(16)
    ]
    for copy in fetches + copies:
        copy.start()
    gain = gain_ref[0:1, :].astype(jnp.float32)
    lanes = pl.ds(pl.multiple_of(sc[34], 256), 256)
    for n in range(8):
        fetches[n].wait()
        own_ref[pl.ds(pl.multiple_of(sc[26 + n], 128), 128), :] = mid_all[128 * n : 128 * (n + 1), lanes]
        wide = mid_all[128 * n : 128 * (n + 1), :].astype(jnp.float32)
        scale = lax.rsqrt(jnp.sum(wide * wide, axis=-1, keepdims=True) / D + eps)
        normed[128 * n : 128 * (n + 1), :] = (wide * scale * gain).astype(jnp.bfloat16)
    for copy in copies:
        copy.wait()
    for n in range(0, 8, 2):
        h = jnp.dot(normed[128 * n : 128 * (n + 2), :], w_up[...], preferred_element_type=jnp.float32)
        h = jnp.square(jnp.maximum(h, 0.0)).astype(jnp.bfloat16)
        for k in range(2):
            h_ref[pl.ds(pl.multiple_of(sc[26 + n + k], 128), 128), :] = h[128 * k : 128 * (k + 1)]


def up(scalars, gain, w, mids):
    vmem = pl.BlockSpec(memory_space=pltpu.VMEM)
    return pl.pallas_call(
        up_kernel,
        out_shape=[
            jax.ShapeDtypeStruct((1024, 1024), jnp.bfloat16),
            jax.ShapeDtypeStruct((1024, 256), jnp.bfloat16),
        ],
        in_specs=[pl.BlockSpec(memory_space=pltpu.SMEM), vmem] + [pl.BlockSpec(memory_space=pltpu.HBM)] * 9,
        out_specs=[vmem, vmem],
        scratch_shapes=[
            pltpu.VMEM((D, 1024), jnp.bfloat16),
            pltpu.VMEM((1024, D), jnp.bfloat16),
            pltpu.VMEM((1024, D), jnp.bfloat16),
            pltpu.SemaphoreType.DMA((24,)),
        ],
        compiler_params=pltpu.CompilerParams(vmem_limit_bytes=40 * 1024 * 1024),
        cost_estimate=pl.CostEstimate(flops=4_300_000_000, bytes_accessed=8_000_000, transcendentals=0),
        name="up",
    )(scalars, gain, *in_hbm([w, *mids]))


def down_kernel(steps, sc, h_ref, w_in, *rest):
    count = len(steps)
    outs, (w_down, sems) = rest[: 2 * count], rest[2 * count :]
    copies = []
    for n, r in enumerate(steps):
        for k in range(4):
            at = pl.multiple_of((sc[36 + r] + k) * 256 + 128, 128)
            copies.append(
                pltpu.make_async_copy(
                    w_in.at[pl.ds(at, 128)], w_down.at[pl.ds(128 * (4 * n + k), 128)], sems.at[4 * n + k]
                )
            )
    for copy in copies:
        copy.start()
    for n in range(count):
        for copy in copies[4 * n : 4 * n + 4]:
            copy.wait()
        for which, out_ref in ((1 - sc[35], outs[2 * n]), (sc[35], outs[2 * n + 1])):
            rows = w_down[pl.ds(pl.multiple_of(512 * n + which * 256, 256), 256), :]
            product = lax.dot_general(
                h_ref[...], rows, (((1,), (1,)), ((), ())), preferred_element_type=jnp.float32
            )
            out_ref[...] = product.astype(out_ref.dtype)


def down(scalars, h, w, steps):
    count = len(steps)
    vmem = pl.BlockSpec(memory_space=pltpu.VMEM)
    return pl.pallas_call(
        functools.partial(down_kernel, steps),
        out_shape=[jax.ShapeDtypeStruct((1024, 256), jnp.bfloat16)] * (2 * count),
        in_specs=[pl.BlockSpec(memory_space=pltpu.SMEM), vmem, pl.BlockSpec(memory_space=pltpu.HBM)],
        out_specs=[vmem] * (2 * count),
        scratch_shapes=[pltpu.VMEM((512 * count, 1024), jnp.bfloat16), pltpu.SemaphoreType.DMA((4 * count,))],
        compiler_params=pltpu.CompilerParams(vmem_limit_bytes=24 * 1024 * 1024),
        cost_estimate=pl.CostEstimate(
            flops=1_100_000_000 * count, bytes_accessed=4_000_000, transcendentals=0
        ),
        name="down",
    )(scalars, h, *in_hbm([w]))


def shifted(value, axis, by):
    n = lax.axis_size(axis)
    return lax.ppermute(value, axis, [(i, (i - by) % n) for i in range(n)])


def partner(value):
    return lax.ppermute(value, "c", [(0, 1), (1, 0)])


def places():
    rows = []
    for d in range(128):
        z, y, x, c = d // 32, d // 8 % 4, d // 2 % 4, d % 2
        mask = [(z & 1) | (k << 1) for k in range(2)]
        row = [y * TOK + c * HALF, mask[c]]
        for r in (0,) + RING:
            for half in (c, 1 - c):
                row += [(y + r) % 4 * TOK + half * HALF, mask[half]]
        order = [((x + r) % 4, k) for r in (0,) + RING for k in (c, 1 - c)]
        row += [xs * 256 + k * 128 for xs, k in order]
        row += [k * 512 + xs * 128 for xs, k in order]
        row += [(2 * x + c) * 256, c] + [(x + r) % 4 * 4 for r in range(4)]
        rows.append(row)
    return np.asarray(rows, np.int32)


PLACES = places()


def body(queries, keys, values, cum_gates, doc_ids, residual, w_out, norm_gain, w_up, w_down):
    z, y, x, c = (lax.axis_index(a) for a in ("z", "y", "x", "c"))
    table = lax.dynamic_slice(jnp.asarray(PLACES), (((z * 4 + y) * 4 + x) * 2 + c, 0), (1, 40)).reshape(40)

    q_t = jnp.transpose(queries * jnp.bfloat16(0.125)).reshape(2, HD, 2, 4, 128)
    q_msg = jnp.transpose(q_t, (0, 2, 3, 1, 4)).reshape(2, 2, Q_ROWS, 128)
    v_t = jnp.transpose(values).reshape(2, HD, 2, 4, 128)
    v_msg = jnp.transpose(v_t, (0, 2, 3, 1, 4)).reshape(2, 2, VROWS, 128)
    k_msg = jnp.transpose(keys.reshape(2, 2, KROWS, 2, HD), (3, 0, 2, 1, 4)).reshape(2, 2, KROWS, 128)
    gates = jnp.transpose(cum_gates).reshape(2, 2, 2, 2, 128)
    hi = lax.reduce_precision(gates, 8, 7)
    mid = lax.reduce_precision(gates - hi, 8, 7)
    low = gates - hi - mid
    three = jnp.transpose(jnp.stack([hi, mid, low]), (1, 2, 4, 3, 0, 5)).reshape(2, 2, 2, 6, 128)
    docs = jnp.broadcast_to(doc_ids.astype(jnp.float32).reshape(1, 2, 4, 128), (2, 2, 4, 128))
    docs = jnp.stack([docs, jnp.zeros_like(docs)], axis=2)
    three = jnp.pad(three, ((0, 0), (0, 0), (0, 0), (0, 2), (0, 0)))
    docs = jnp.pad(docs, ((0, 0), (0, 0), (0, 0), (0, 4), (0, 0)))
    g_msg = jnp.concatenate([three, docs], axis=3).reshape(2, 2, GROWS, 128).astype(jnp.bfloat16)
    messages = jnp.concatenate([k_msg, v_msg, g_msg, q_msg], axis=2)

    received = []
    for step in range(4):
        pairs = []
        for zs in range(4):
            for cs in range(2):
                j = 2 * cs + ((zs & 1) ^ (step & 1))
                cd = (zs >> 1) ^ (step >> 1)
                pairs.append((zs * 2 + cs, j * 2 + cd))
        head = (z & 1) ^ (step & 1)
        half = (z >> 1) ^ (step >> 1)
        message = lax.dynamic_slice(messages, (head, half, 0, 0), (1, 1, KV_ROWS + Q_ROWS, 128))[0, 0]
        received.append(lax.ppermute(message, ("z", "c"), pairs))
    gain_row = jnp.pad(norm_gain[None], ((0, 7), (0, D - 256)))
    w_msg = jnp.concatenate([w_out, gain_row], axis=0)
    w_mine = [w_msg] + [shifted(w_msg, "x", r) for r in RING]

    qt = jnp.stack([r[KV_ROWS:] for r in received])
    kv_own = jnp.stack([r[:KV_ROWS] for r in received])

    kv_mine = [kv_own] + [shifted(kv_own, "y", r) for r in RING]

    kv_own, residual, w_up, w_down = lax.optimization_barrier((kv_own, residual, w_up, w_down))
    both = jnp.concatenate([w_up, jnp.transpose(w_down)], axis=0)

    docs_own = kv_own[:, KROWS + VROWS + 8 : KROWS + VROWS + 16].astype(jnp.float32)
    zeros_q = (HALF - jnp.sum(docs_own, axis=(1, 2))).astype(jnp.int32)

    kv_near = partner(kv_own)
    state = attend(table, zeros_q, qt, [kv_own, kv_near], (), True, False)
    res = lax.all_to_all(residual.reshape(8, 128, 256), ("c", "x"), 0, 0, tiled=True)
    kv_mine[1:], state, both = lax.optimization_barrier((kv_mine[1:], state, both))
    both = lax.all_gather(both, ("z", "y"), axis=0, tiled=True)
    kv_other = [None] + [partner(piece) for piece in kv_mine[1:]]
    pieces = [piece for pair in zip(kv_mine[1:], kv_other[1:]) for piece in pair]
    out = attend(table, zeros_q, qt, pieces, state, False, True)

    w_mine, res, out = lax.optimization_barrier((w_mine, res, out))
    w_pieces = [w for mine in w_mine for w in (mine, partner(mine))]

    attended = lax.all_to_all(out, ("x", "z"), 0, 0, tiled=True)

    middle, gain = dense(table, attended, res, w_pieces)

    mid_mine = [middle] + [shifted(middle, "x", r) for r in RING]
    mids = [m for mine in mid_mine for m in (mine, partner(mine))]
    hidden, middle_own = up(table, gain, both, mids)

    parts = {}
    for steps in ((2,), (0,), (1, 3)):
        products = down(table, hidden, both, steps)
        for n, r in enumerate(steps):
            parts[r] = products[2 * n + 1].astype(jnp.float32) + partner(products[2 * n]).astype(jnp.float32)
    total = middle_own.astype(jnp.float32) + parts[0]
    for r in (2, 1, 3):
        total = total + shifted(parts[r].astype(jnp.bfloat16), "x", -r).astype(jnp.float32)
    return total.astype(jnp.bfloat16)


def solution(mesh):
    split = Mesh(mesh.devices.reshape(4, 4, 4, 2), ("z", "y", "x", "c"))
    sp, tp = ("z", "y"), ("x", "c")
    in_specs = (
        P(sp, tp),
        P(sp, tp),
        P(sp, tp),
        P(sp, tp),
        P(sp),
        P(sp, tp),
        P(tp, None),
        P(tp),
        P(sp, tp),
        P(tp, sp),
    )
    return jax.shard_map(body, mesh=split, in_specs=in_specs, out_specs=P(sp, tp), check_vma=False)
```

```python
import functools

import jax
import jax.numpy as jnp
import numpy as np
from jax import lax
from jax.experimental import pallas as pl
from jax.experimental.pallas import tpu as pltpu
from jax.sharding import Mesh, PartitionSpec as P

D = 2048
HD = 64
TOK = 1024
HALF = 512
KROWS = 256
VROWS = 256
GROWS = 32
KV_ROWS = KROWS + VROWS + GROWS
Q_ROWS = 256

eps = 1e-06
far_below = -1e30
lowest = -1e29
RING = (1, 3, 2)


def in_hbm(arrays):
    return [pltpu.with_memory_space_constraint(a, pltpu.HBM) for a in arrays]


def pack_kernel(tab, *rest):
    arrays, outs, (q_ref, v_ref, k_ref, g_ref, d_ref, msgs, sems) = rest[:5], rest[5:9], rest[9:]
    copies = [
        pltpu.make_async_copy(a, to, sems.at[n]) for n, (a, to) in enumerate(zip(arrays, (q_ref, v_ref, k_ref, g_ref, d_ref)))
    ]
    for copy in copies:
        copy.start()
    for copy in copies:
        copy.wait()
    q_t = (q_ref[...].astype(jnp.float32) * 0.125).T.astype(jnp.bfloat16)
    v_t = v_ref[...].astype(jnp.float32).T.astype(jnp.bfloat16)
    docs = d_ref[...].astype(jnp.float32)
    hi = g_ref[...].astype(jnp.bfloat16).astype(jnp.float32)
    rest_of = g_ref[...] - hi
    mid = rest_of.astype(jnp.bfloat16).astype(jnp.float32)
    low = (rest_of - mid).astype(jnp.bfloat16).astype(jnp.float32)

    def blank(rows):
        return jnp.zeros((rows, 128), jnp.float32)

    def chunk(a, row, n):
        return a[row : row + 1, 128 * n : 128 * (n + 1)]

    for head in range(2):
        lanes = slice(64 * head, 64 * (head + 1))
        for half in range(2):
            m = 2 * head + half
            at = HALF * half
            msgs[m, 0:KROWS, :] = jnp.concatenate(
                [k_ref[at : at + 256, lanes], k_ref[at + 256 : at + 512, lanes]], axis=1
            )
            for n in range(4):
                to = KROWS + 64 * n
                msgs[m, to : to + 64, :] = v_t[lanes, at + 128 * n : at + 128 * (n + 1)]
                tokens = at + 128 * n
                to = KV_ROWS + 64 * n
                msgs[m, to : to + 64, :] = q_t[lanes, tokens : tokens + 128]
            for k in range(2):
                rows = [chunk(a, head, 4 * half + k + 2 * side) for side in range(2) for a in (hi, mid, low)]
                rows.append(blank(2))
                if k == 0:
                    rows += [chunk(docs, 0, 4 * half + n) for n in range(4)] + [blank(4)]
                else:
                    rows.append(blank(8))
                to = KROWS + VROWS + 16 * k
                msgs[m, to : to + 16, :] = jnp.concatenate(rows, axis=0).astype(jnp.bfloat16)
    for step in range(4):
        outs[step][...] = msgs[tab[40 + step]]


def pack(table, q, k, v, g, d):
    vmem = pl.BlockSpec(memory_space=pltpu.VMEM)
    rows = KV_ROWS + Q_ROWS
    return pl.pallas_call(
        pack_kernel,
        out_shape=[jax.ShapeDtypeStruct((rows, 128), jnp.bfloat16)] * 4,
        in_specs=[pl.BlockSpec(memory_space=pltpu.SMEM)] + [pl.BlockSpec(memory_space=pltpu.HBM)] * 5,
        out_specs=[vmem] * 4,
        scratch_shapes=[pltpu.VMEM((TOK, 128), jnp.bfloat16)] * 3
        + [
            pltpu.VMEM((2, TOK), jnp.float32),
            pltpu.VMEM((1, TOK), jnp.int32),
            pltpu.VMEM((4, rows, 128), jnp.bfloat16),
            pltpu.SemaphoreType.DMA((5,)),
        ],
        compiler_params=pltpu.CompilerParams(vmem_limit_bytes=16 * 1024 * 1024),
        cost_estimate=pl.CostEstimate(flops=10_000_000, bytes_accessed=2_000_000, transcendentals=0),
        name="pack",
    )(table, *in_hbm([q, v, k, g, d]))


DIMS = (((1,), (0,)), ((), ()))


def score(i, pq, kv, ke, qa, qb, s_ref):
    keys = jnp.concatenate([kv[i, 0:KROWS, :], ke[i]], axis=1)
    for j in range(2):
        for part, q_ref in enumerate((qa, qb)):
            s_ref[j, 256 * part : 256 * (part + 1), :] = lax.dot_general(
                keys, q_ref[pq, :, 256 * j : 256 * (j + 1)], DIMS, preferred_element_type=jnp.float32
            )


def hide(s_ref, ahead, k_zero, q_zero):
    for j in range(2):
        for part in range(2):
            row = lax.broadcasted_iota(jnp.int32, (256, 256), 0)
            lane = lax.broadcasted_iota(jnp.int32, (256, 256), 1)
            seen = (row - lane <= ahead + 256 * (j - part)) & (
                (row >= k_zero - 256 * part) | (lane < q_zero - 256 * j)
            )
            at = slice(256 * part, 256 * (part + 1))
            s_ref[j, at, :] = jnp.where(seen, s_ref[j, at, :], far_below)


def weigh(pq, s_ref, p_ref, m_ref, l_ref, shrink_ref):
    for j in range(2):
        cols = slice(256 * j, 256 * (j + 1))
        top = jnp.max(s_ref[j, 0:64, :].reshape(8, 8, 256), axis=0)
        for n in range(1, 8):
            top = jnp.maximum(top, jnp.max(s_ref[j, 64 * n : 64 * (n + 1), :].reshape(8, 8, 256), axis=0))
        m_old = m_ref[pq, :, cols]
        m_new = jnp.maximum(m_old, jnp.max(top, axis=0, keepdims=True))
        shrink = jnp.exp(m_old - m_new)
        m_ref[pq, :, cols] = m_new
        shrink_ref[:, cols] = shrink
        sums = jnp.zeros((8, 256), jnp.float32)
        for n in range(8):
            p = jnp.exp(s_ref[j, 64 * n : 64 * (n + 1), :] - m_new)
            sums = sums + jnp.sum(p.reshape(8, 8, 256), axis=0)
            p_ref[j, 64 * n : 64 * (n + 1), :] = p.astype(jnp.bfloat16)
        l_ref[pq, :, cols] = l_ref[pq, :, cols] * shrink + jnp.sum(sums, axis=0, keepdims=True)


def blend(i, pq, kv, p_ref, shrink_ref, acc_ref):
    values = jnp.concatenate([kv[i, KROWS + 64 * n : KROWS + 64 * (n + 1), :] for n in range(4)], axis=1)
    for j in range(2):
        cols = slice(256 * j, 256 * (j + 1))
        product = lax.dot_general(values, p_ref[j], DIMS, preferred_element_type=jnp.float32)
        acc_ref[pq, :, cols] = acc_ref[pq, :, cols] * shrink_ref[:, cols] + product


def attend_kernel(n_arr, first, last, tab, zeros_q, qt_ref, *rest):
    kv_in, rest = rest[:n_arr], rest[n_arr:]
    if first:
        state_in = ()
    else:
        state_in, rest = rest[:3], rest[3:]
    if last:
        out_ref, rest = rest[0], rest[1:]
    m_ref, l_ref, acc_ref, kv, ke, qa, qb, s_a, s_b, p_a, p_b, shrink_a, shrink_b, zero_s, todo, sems = rest
    at_keys = 2 if first else 6
    copies = [
        pltpu.make_async_copy(kv_in[n], kv.at[pl.ds(4 * n, 4)], sems.at[n]) for n in range(n_arr)
    ]
    for copy in copies:
        copy.start()
    if first:
        m_ref[...] = jnp.full(m_ref.shape, lowest, jnp.float32)
        l_ref[...] = jnp.zeros(l_ref.shape, jnp.float32)
        acc_ref[...] = jnp.zeros(acc_ref.shape, jnp.float32)
    else:
        m_ref[...] = state_in[0][...]
        l_ref[...] = state_in[1][...]
        acc_ref[...] = state_in[2][...]
    row = lax.broadcasted_iota(jnp.int32, (128, HALF), 0)
    minus_a = jnp.where(row < 3, -1.0, 0.0).astype(jnp.bfloat16)
    minus_b = jnp.where((row >= 3) & (row < 6), -1.0, 0.0).astype(jnp.bfloat16)
    zeros = jnp.zeros((64, HALF), jnp.bfloat16)
    for pq in range(4):
        q = jnp.concatenate([qt_ref[pq, 64 * n : 64 * (n + 1), :] for n in range(4)], axis=1)
        qa[pq, 0:64, :] = q
        qa[pq, 64:128, :] = zeros
        qa[pq, 128:256, :] = minus_a
        qb[pq, 0:64, :] = zeros
        qb[pq, 64:128, :] = q
        qb[pq, 128:256, :] = minus_b
    for copy in copies:
        copy.wait()
    blank = jnp.zeros((112, 128), jnp.float32)

    def prepare(n, carry):
        for k in range(4):
            i = 4 * n + k
            g = kv[i, KROWS + VROWS : KV_ROWS, :].astype(jnp.float32)
            for half in range(2):
                turned = jnp.concatenate([g[16 * half : 16 * (half + 1)], blank], axis=0).T
                ke[i, 128 * half : 128 * (half + 1), :] = turned.astype(jnp.bfloat16)
            zero_s[i] = HALF - jnp.sum(g[8:16]).astype(jnp.int32)
        return carry

    lax.fori_loop(0, n_arr, prepare, 0)

    def list_keys(i, count):
        arr = i // 4
        k_start = ((i % 4) ^ tab[at_keys + 1 + 2 * arr]) * 4096 + tab[at_keys + 2 * arr]
        k_zero = zero_s[i]
        for pq in range(4):
            ahead = (pq ^ tab[1]) * 4096 + tab[0] - k_start
            q_zero = zeros_q[pq]
            live = (ahead > -HALF) & jnp.logical_not((k_zero == HALF) & (q_zero == 0))
            full = (ahead >= HALF) & ((k_zero == 0) | (q_zero == HALF))
            todo[count, 0] = i
            todo[count, 1] = pq
            todo[count, 2] = ahead
            todo[count, 3] = jnp.where(full, 0, 1)
            count = count + live.astype(jnp.int32)
        return count

    count = lax.fori_loop(0, 4 * n_arr, list_keys, 0)
    for extra in range(2):
        todo[count + extra, 0] = 0
        todo[count + extra, 1] = 0
        todo[count + extra, 2] = -100000
        todo[count + extra, 3] = 1

    p_b[...] = jnp.zeros(p_b.shape, jnp.bfloat16)
    shrink_b[...] = jnp.ones(shrink_b.shape, jnp.float32)
    score(todo[0, 0], todo[0, 1], kv, ke, qa, qb, s_a)

    def step(t, now, later):
        s_now, p_now, shrink_now = now
        s_later, p_later, shrink_later = later
        before = jnp.maximum(t - 1, 0)

        @pl.when(todo[t, 3] == 1)
        def _():
            hide(s_now, todo[t, 2], zero_s[todo[t, 0]], zeros_q[todo[t, 1]])

        score(todo[t + 1, 0], todo[t + 1, 1], kv, ke, qa, qb, s_later)
        weigh(todo[t, 1], s_now, p_now, m_ref, l_ref, shrink_now)
        blend(todo[before, 0], todo[before, 1], kv, p_later, shrink_later, acc_ref)

    def two_steps(n, carry):
        side_a, side_b = (s_a, p_a, shrink_a), (s_b, p_b, shrink_b)
        step(2 * n, side_a, side_b)
        step(2 * n + 1, side_b, side_a)
        return carry

    rounds = (count + 1) // 2
    lax.fori_loop(0, rounds, two_steps, 0)

    @pl.when(rounds > 0)
    def _():
        at = 2 * rounds - 1
        blend(todo[at, 0], todo[at, 1], kv, p_b, shrink_b, acc_ref)

    if last:

        def finish(pq, carry):
            out = (acc_ref[pq] / l_ref[pq]).astype(jnp.bfloat16)
            block = pq ^ tab[1]
            for quarter in range(4):
                out_ref[quarter * 4 + block] = out[:, 128 * quarter : 128 * (quarter + 1)]
            return carry

        lax.fori_loop(0, 4, finish, 0)


def attend(table, zeros_q, qt, arrays, state, first, last):
    n_arr = len(arrays)
    vmem = pl.BlockSpec(memory_space=pltpu.VMEM)
    shapes = [
        jax.ShapeDtypeStruct((4, 1, HALF), jnp.float32),
        jax.ShapeDtypeStruct((4, 1, HALF), jnp.float32),
        jax.ShapeDtypeStruct((4, HD, HALF), jnp.float32),
    ]
    scratch = [
        pltpu.VMEM((4 * n_arr, KV_ROWS, 128), jnp.bfloat16),
        pltpu.VMEM((4 * n_arr, 256, 128), jnp.bfloat16),
        pltpu.VMEM((4, 256, HALF), jnp.bfloat16),
        pltpu.VMEM((4, 256, HALF), jnp.bfloat16),
        pltpu.VMEM((2, HALF, 256), jnp.float32),
        pltpu.VMEM((2, HALF, 256), jnp.float32),
        pltpu.VMEM((2, HALF, 256), jnp.bfloat16),
        pltpu.VMEM((2, HALF, 256), jnp.bfloat16),
        pltpu.VMEM((1, HALF), jnp.float32),
        pltpu.VMEM((1, HALF), jnp.float32),
        pltpu.SMEM((4 * n_arr,), jnp.int32),
        pltpu.SMEM((16 * n_arr + 2, 4), jnp.int32),
        pltpu.SemaphoreType.DMA((n_arr,)),
    ]
    if last:
        out_shape = jax.ShapeDtypeStruct((16, HD, 128), jnp.bfloat16)
        out_specs = vmem
        scratch = [pltpu.VMEM(s.shape, s.dtype) for s in shapes] + scratch
    else:
        out_shape = shapes
        out_specs = [vmem] * 3
    state = () if first else tuple(state)
    return pl.pallas_call(
        functools.partial(attend_kernel, n_arr, first, last),
        out_shape=out_shape,
        in_specs=[pl.BlockSpec(memory_space=pltpu.SMEM)] * 2
        + [vmem]
        + [pl.BlockSpec(memory_space=pltpu.HBM)] * n_arr
        + [vmem] * len(state),
        out_specs=out_specs,
        scratch_shapes=scratch,
        compiler_params=pltpu.CompilerParams(vmem_limit_bytes=40 * 1024 * 1024),
        cost_estimate=pl.CostEstimate(
            flops=4_000_000_000 * n_arr, bytes_accessed=1_000_000 * n_arr, transcendentals=0
        ),
        name="attend_first" if first else ("attend_last" if last else "attend_more"),
    )(table, zeros_q, qt, *in_hbm(arrays), *state)


def dense_kernel(sc, att_ref, res_ref, *rest):
    w_in, (mid_ref, gain_ref, w_all, sems) = rest[:8], rest[8:]
    copies = []
    for n in range(8):
        at = pl.multiple_of(sc[18 + n], 128)
        lanes = pl.ds(pl.multiple_of(sc[18 + n] * 2, 256), 256)
        copies.append(pltpu.make_async_copy(w_in[n].at[pl.ds(0, 128)], w_all.at[pl.ds(at, 128)], sems.at[n]))
        copies.append(
            pltpu.make_async_copy(w_in[n].at[pl.ds(128, 8), pl.ds(0, 256)], gain_ref.at[:, lanes], sems.at[8 + n])
        )
    for copy in copies:
        copy.start()
    for copy in copies:
        copy.wait()
    att = att_ref[...].reshape(1024, 128)
    for n in range(8):
        tp = 2 * (n % 4) + n // 4
        cols = slice(256 * tp, 256 * (tp + 1))
        mixed = lax.dot_general(
            att, w_all[:, cols], (((0,), (0,)), ((), ())), preferred_element_type=jnp.float32
        )
        mid_ref[:, cols] = (res_ref[n].astype(jnp.float32) + mixed).astype(jnp.bfloat16)


def dense(scalars, att, res, pieces):
    vmem = pl.BlockSpec(memory_space=pltpu.VMEM)
    return pl.pallas_call(
        dense_kernel,
        out_shape=[
            jax.ShapeDtypeStruct((128, D), jnp.bfloat16),
            jax.ShapeDtypeStruct((8, D), jnp.bfloat16),
        ],
        in_specs=[pl.BlockSpec(memory_space=pltpu.SMEM), vmem, vmem] + [pl.BlockSpec(memory_space=pltpu.HBM)] * 8,
        out_specs=[vmem, vmem],
        scratch_shapes=[pltpu.VMEM((1024, D), jnp.bfloat16), pltpu.SemaphoreType.DMA((16,))],
        compiler_params=pltpu.CompilerParams(vmem_limit_bytes=24 * 1024 * 1024),
        cost_estimate=pl.CostEstimate(flops=1_000_000_000, bytes_accessed=4_000_000, transcendentals=0),
        name="dense",
    )(scalars, att, res, *in_hbm(pieces))


def up_kernel(sc, gain_ref, w_in, *rest):
    mids, (h_ref, own_ref, w_up, mid_all, normed, sems) = rest[:8], rest[8:]
    fetches = [pltpu.make_async_copy(mids[n], mid_all.at[pl.ds(128 * n, 128)], sems.at[16 + n]) for n in range(8)]
    copies = [
        pltpu.make_async_copy(w_in.at[pl.ds(256 * n, 128)], w_up.at[pl.ds(128 * n, 128)], sems.at[n]) for n in range(16)
    ]
    for copy in fetches + copies:
        copy.start()
    gain = gain_ref[0:1, :].astype(jnp.float32)
    lanes = pl.ds(pl.multiple_of(sc[34], 256), 256)
    for n in range(8):
        fetches[n].wait()
        own_ref[pl.ds(pl.multiple_of(sc[26 + n], 128), 128), :] = mid_all[128 * n : 128 * (n + 1), lanes]
        wide = mid_all[128 * n : 128 * (n + 1), :].astype(jnp.float32)
        scale = lax.rsqrt(jnp.sum(wide * wide, axis=-1, keepdims=True) / D + eps)
        normed[128 * n : 128 * (n + 1), :] = (wide * scale * gain).astype(jnp.bfloat16)
    for copy in copies:
        copy.wait()
    for n in range(0, 8, 2):
        h = jnp.dot(normed[128 * n : 128 * (n + 2), :], w_up[...], preferred_element_type=jnp.float32)
        h = jnp.square(jnp.maximum(h, 0.0)).astype(jnp.bfloat16)
        for k in range(2):
            h_ref[pl.ds(pl.multiple_of(sc[26 + n + k], 128), 128), :] = h[128 * k : 128 * (k + 1)]


def up(scalars, gain, w, mids):
    vmem = pl.BlockSpec(memory_space=pltpu.VMEM)
    return pl.pallas_call(
        up_kernel,
        out_shape=[
            jax.ShapeDtypeStruct((1024, 1024), jnp.bfloat16),
            jax.ShapeDtypeStruct((1024, 256), jnp.bfloat16),
        ],
        in_specs=[pl.BlockSpec(memory_space=pltpu.SMEM), vmem] + [pl.BlockSpec(memory_space=pltpu.HBM)] * 9,
        out_specs=[vmem, vmem],
        scratch_shapes=[
            pltpu.VMEM((D, 1024), jnp.bfloat16),
            pltpu.VMEM((1024, D), jnp.bfloat16),
            pltpu.VMEM((1024, D), jnp.bfloat16),
            pltpu.SemaphoreType.DMA((24,)),
        ],
        compiler_params=pltpu.CompilerParams(vmem_limit_bytes=40 * 1024 * 1024),
        cost_estimate=pl.CostEstimate(flops=4_300_000_000, bytes_accessed=8_000_000, transcendentals=0),
        name="up",
    )(scalars, gain, *in_hbm([w, *mids]))


def down_kernel(steps, sc, h_ref, w_in, *rest):
    count = len(steps)
    outs, (w_down, sems) = rest[: 2 * count], rest[2 * count :]
    copies = []
    for n, r in enumerate(steps):
        for k in range(4):
            at = pl.multiple_of((sc[36 + r] + k) * 256 + 128, 128)
            copies.append(
                pltpu.make_async_copy(
                    w_in.at[pl.ds(at, 128)], w_down.at[pl.ds(128 * (4 * n + k), 128)], sems.at[4 * n + k]
                )
            )
    for copy in copies:
        copy.start()
    for n in range(count):
        for copy in copies[4 * n : 4 * n + 4]:
            copy.wait()
        for which, out_ref in ((1 - sc[35], outs[2 * n]), (sc[35], outs[2 * n + 1])):
            rows = w_down[pl.ds(pl.multiple_of(512 * n + which * 256, 256), 256), :]
            product = lax.dot_general(
                h_ref[...], rows, (((1,), (1,)), ((), ())), preferred_element_type=jnp.float32
            )
            out_ref[...] = product.astype(out_ref.dtype)


def down(scalars, h, w, steps):
    count = len(steps)
    vmem = pl.BlockSpec(memory_space=pltpu.VMEM)
    return pl.pallas_call(
        functools.partial(down_kernel, steps),
        out_shape=[jax.ShapeDtypeStruct((1024, 256), jnp.bfloat16)] * (2 * count),
        in_specs=[pl.BlockSpec(memory_space=pltpu.SMEM), vmem, pl.BlockSpec(memory_space=pltpu.HBM)],
        out_specs=[vmem] * (2 * count),
        scratch_shapes=[pltpu.VMEM((512 * count, 1024), jnp.bfloat16), pltpu.SemaphoreType.DMA((4 * count,))],
        compiler_params=pltpu.CompilerParams(vmem_limit_bytes=24 * 1024 * 1024),
        cost_estimate=pl.CostEstimate(
            flops=1_100_000_000 * count, bytes_accessed=4_000_000, transcendentals=0
        ),
        name="down",
    )(scalars, h, *in_hbm([w]))


def shifted(value, axis, by):
    n = lax.axis_size(axis)
    return lax.ppermute(value, axis, [(i, (i - by) % n) for i in range(n)])


def partner(value):
    return lax.ppermute(value, "c", [(0, 1), (1, 0)])


def places():
    rows = []
    for d in range(128):
        z, y, x, c = d // 32, d // 8 % 4, d // 2 % 4, d % 2
        mask = [(z & 1) | (k << 1) for k in range(2)]
        row = [y * TOK + c * HALF, mask[c]]
        for r in (0,) + RING:
            for half in (c, 1 - c):
                row += [(y + r) % 4 * TOK + half * HALF, mask[half]]
        order = [((x + r) % 4, k) for r in (0,) + RING for k in (c, 1 - c)]
        row += [xs * 256 + k * 128 for xs, k in order]
        row += [k * 512 + xs * 128 for xs, k in order]
        row += [(2 * x + c) * 256, c] + [(x + r) % 4 * 4 for r in range(4)]
        row += [2 * ((z & 1) ^ (k & 1)) + ((z >> 1) ^ (k >> 1)) for k in range(4)]
        rows.append(row)
    return np.asarray(rows, np.int32)


PLACES = places()


def body(queries, keys, values, cum_gates, doc_ids, residual, w_out, norm_gain, w_up, w_down):
    z, y, x, c = (lax.axis_index(a) for a in ("z", "y", "x", "c"))
    table = lax.dynamic_slice(jnp.asarray(PLACES), (((z * 4 + y) * 4 + x) * 2 + c, 0), (1, 44)).reshape(44)

    messages = pack(table, queries, keys, values, jnp.transpose(cum_gates), doc_ids.reshape(1, TOK))

    received = []
    for step in range(4):
        pairs = []
        for zs in range(4):
            for cs in range(2):
                j = 2 * cs + ((zs & 1) ^ (step & 1))
                cd = (zs >> 1) ^ (step >> 1)
                pairs.append((zs * 2 + cs, j * 2 + cd))
        received.append(lax.ppermute(messages[step], ("z", "c"), pairs))
    gain_row = jnp.pad(norm_gain[None], ((0, 7), (0, D - 256)))
    w_msg = jnp.concatenate([w_out, gain_row], axis=0)
    w_mine = [w_msg] + [shifted(w_msg, "x", r) for r in RING]

    qt = jnp.stack([r[KV_ROWS:] for r in received])
    kv_own = jnp.stack([r[:KV_ROWS] for r in received])

    kv_mine = [kv_own] + [shifted(kv_own, "y", r) for r in RING]

    kv_own, residual, w_up, w_down = lax.optimization_barrier((kv_own, residual, w_up, w_down))
    both = jnp.concatenate([w_up, jnp.transpose(w_down)], axis=0)

    docs_own = kv_own[:, KROWS + VROWS + 8 : KROWS + VROWS + 16].astype(jnp.float32)
    zeros_q = (HALF - jnp.sum(docs_own, axis=(1, 2))).astype(jnp.int32)

    kv_near = partner(kv_own)
    state = attend(table, zeros_q, qt, [kv_own, kv_near], (), True, False)
    res = lax.all_to_all(residual.reshape(8, 128, 256), ("c", "x"), 0, 0, tiled=True)
    kv_mine[1:], state, both = lax.optimization_barrier((kv_mine[1:], state, both))
    both = lax.all_gather(both, ("z", "y"), axis=0, tiled=True)
    kv_other = [None] + [partner(piece) for piece in kv_mine[1:]]
    pieces = [piece for pair in zip(kv_mine[1:], kv_other[1:]) for piece in pair]
    out = attend(table, zeros_q, qt, pieces, state, False, True)

    w_mine, res, out = lax.optimization_barrier((w_mine, res, out))
    w_pieces = [w for mine in w_mine for w in (mine, partner(mine))]

    attended = lax.all_to_all(out, ("x", "z"), 0, 0, tiled=True)

    middle, gain = dense(table, attended, res, w_pieces)

    mid_mine = [middle] + [shifted(middle, "x", r) for r in RING]
    mids = [m for mine in mid_mine for m in (mine, partner(mine))]
    hidden, middle_own = up(table, gain, both, mids)

    parts = {}
    for steps in ((2,), (0,), (1, 3)):
        products = down(table, hidden, both, steps)
        for n, r in enumerate(steps):
            parts[r] = products[2 * n + 1].astype(jnp.float32) + partner(products[2 * n]).astype(jnp.float32)
    total = middle_own.astype(jnp.float32) + parts[0]
    for r in (2, 1, 3):
        total = total + shifted(parts[r].astype(jnp.bfloat16), "x", -r).astype(jnp.float32)
    return total.astype(jnp.bfloat16)


def solution(mesh):
    split = Mesh(mesh.devices.reshape(4, 4, 4, 2), ("z", "y", "x", "c"))
    sp, tp = ("z", "y"), ("x", "c")
    in_specs = (
        P(sp, tp),
        P(sp, tp),
        P(sp, tp),
        P(sp, tp),
        P(sp),
        P(sp, tp),
        P(tp, None),
        P(tp),
        P(sp, tp),
        P(tp, sp),
    )
    return jax.shard_map(body, mesh=split, in_specs=in_specs, out_specs=P(sp, tp), check_vma=False)
```

```python
import functools

import jax
import jax.numpy as jnp
import numpy as np
from jax import lax
from jax.experimental import pallas as pl
from jax.experimental.pallas import tpu as pltpu
from jax.sharding import Mesh, PartitionSpec as P

D = 2048
HD = 64
TOK = 1024
HALF = 512
KROWS = 256
VROWS = 256
GROWS = 32
KV_ROWS = KROWS + VROWS + GROWS
Q_ROWS = 256

eps = 1e-06
far_below = -1e30
lowest = -1e29
RING = (1, 3, 2)


def in_hbm(arrays):
    return [pltpu.with_memory_space_constraint(a, pltpu.HBM) for a in arrays]


def pack_kernel(tab, *rest):
    arrays, outs, (q_ref, v_ref, k_ref, g_ref, d_ref, msgs, sems) = rest[:5], rest[5:9], rest[9:]
    copies = [
        pltpu.make_async_copy(a, to, sems.at[n]) for n, (a, to) in enumerate(zip(arrays, (q_ref, v_ref, k_ref, g_ref, d_ref)))
    ]
    for copy in copies:
        copy.start()
    for copy in copies:
        copy.wait()
    q_t = (q_ref[...].astype(jnp.float32) * 0.125).T.astype(jnp.bfloat16)
    v_t = v_ref[...].astype(jnp.float32).T.astype(jnp.bfloat16)
    docs = d_ref[...].astype(jnp.float32)
    hi = g_ref[...].astype(jnp.bfloat16).astype(jnp.float32)
    rest_of = g_ref[...] - hi
    mid = rest_of.astype(jnp.bfloat16).astype(jnp.float32)
    low = (rest_of - mid).astype(jnp.bfloat16).astype(jnp.float32)

    def blank(rows):
        return jnp.zeros((rows, 128), jnp.float32)

    def chunk(a, row, n):
        return a[row : row + 1, 128 * n : 128 * (n + 1)]

    for head in range(2):
        lanes = slice(64 * head, 64 * (head + 1))
        for half in range(2):
            m = 2 * head + half
            at = HALF * half
            msgs[m, 0:KROWS, :] = jnp.concatenate(
                [k_ref[at : at + 256, lanes], k_ref[at + 256 : at + 512, lanes]], axis=1
            )
            for n in range(4):
                to = KROWS + 64 * n
                msgs[m, to : to + 64, :] = v_t[lanes, at + 128 * n : at + 128 * (n + 1)]
                tokens = at + 128 * n
                to = KV_ROWS + 64 * n
                msgs[m, to : to + 64, :] = q_t[lanes, tokens : tokens + 128]
            for k in range(2):
                rows = [chunk(a, head, 4 * half + k + 2 * side) for side in range(2) for a in (hi, mid, low)]
                rows.append(blank(2))
                if k == 0:
                    rows += [chunk(docs, 0, 4 * half + n) for n in range(4)] + [blank(4)]
                else:
                    rows.append(blank(8))
                to = KROWS + VROWS + 16 * k
                msgs[m, to : to + 16, :] = jnp.concatenate(rows, axis=0).astype(jnp.bfloat16)
    for step in range(4):
        outs[step][...] = msgs[tab[40 + step]]


def pack(table, q, k, v, g, d):
    vmem = pl.BlockSpec(memory_space=pltpu.VMEM)
    rows = KV_ROWS + Q_ROWS
    return pl.pallas_call(
        pack_kernel,
        out_shape=[jax.ShapeDtypeStruct((rows, 128), jnp.bfloat16)] * 4,
        in_specs=[pl.BlockSpec(memory_space=pltpu.SMEM)] + [pl.BlockSpec(memory_space=pltpu.HBM)] * 5,
        out_specs=[vmem] * 4,
        scratch_shapes=[pltpu.VMEM((TOK, 128), jnp.bfloat16)] * 3
        + [
            pltpu.VMEM((2, TOK), jnp.float32),
            pltpu.VMEM((1, TOK), jnp.int32),
            pltpu.VMEM((4, rows, 128), jnp.bfloat16),
            pltpu.SemaphoreType.DMA((5,)),
        ],
        compiler_params=pltpu.CompilerParams(vmem_limit_bytes=16 * 1024 * 1024),
        cost_estimate=pl.CostEstimate(flops=10_000_000, bytes_accessed=2_000_000, transcendentals=0),
        name="pack",
    )(table, *in_hbm([q, v, k, g, d]))


DIMS = (((1,), (0,)), ((), ()))


def score(i, pq, kv, ke, qa, qb, s_ref):
    keys = jnp.concatenate([kv[i, 0:KROWS, :], ke[i]], axis=1)
    for j in range(2):
        for part, q_ref in enumerate((qa, qb)):
            s_ref[j, 256 * part : 256 * (part + 1), :] = lax.dot_general(
                keys, q_ref[pq, :, 256 * j : 256 * (j + 1)], DIMS, preferred_element_type=jnp.float32
            )


def hide(s_ref, ahead, k_zero, q_zero):
    for j in range(2):
        for part in range(2):
            row = lax.broadcasted_iota(jnp.int32, (256, 256), 0)
            lane = lax.broadcasted_iota(jnp.int32, (256, 256), 1)
            seen = (row - lane <= ahead + 256 * (j - part)) & (
                (row >= k_zero - 256 * part) | (lane < q_zero - 256 * j)
            )
            at = slice(256 * part, 256 * (part + 1))
            s_ref[j, at, :] = jnp.where(seen, s_ref[j, at, :], far_below)


def weigh(pq, s_ref, p_ref, m_ref, l_ref, shrink_ref):
    for j in range(2):
        cols = slice(256 * j, 256 * (j + 1))
        top = jnp.max(s_ref[j, 0:64, :].reshape(8, 8, 256), axis=0)
        for n in range(1, 8):
            top = jnp.maximum(top, jnp.max(s_ref[j, 64 * n : 64 * (n + 1), :].reshape(8, 8, 256), axis=0))
        m_old = m_ref[pq, :, cols]
        m_new = jnp.maximum(m_old, jnp.max(top, axis=0, keepdims=True))
        shrink = jnp.exp(m_old - m_new)
        m_ref[pq, :, cols] = m_new
        shrink_ref[:, cols] = shrink
        sums = jnp.zeros((8, 256), jnp.float32)
        for n in range(8):
            p = jnp.exp(s_ref[j, 64 * n : 64 * (n + 1), :] - m_new)
            sums = sums + jnp.sum(p.reshape(8, 8, 256), axis=0)
            p_ref[j, 64 * n : 64 * (n + 1), :] = p.astype(jnp.bfloat16)
        l_ref[pq, :, cols] = l_ref[pq, :, cols] * shrink + jnp.sum(sums, axis=0, keepdims=True)


def blend(i, pq, kv, p_ref, shrink_ref, acc_ref):
    values = jnp.concatenate([kv[i, KROWS + 64 * n : KROWS + 64 * (n + 1), :] for n in range(4)], axis=1)
    for j in range(2):
        cols = slice(256 * j, 256 * (j + 1))
        product = lax.dot_general(values, p_ref[j], DIMS, preferred_element_type=jnp.float32)
        acc_ref[pq, :, cols] = acc_ref[pq, :, cols] * shrink_ref[:, cols] + product


def attend_kernel(n_arr, first, last, tab, zeros_q, qt_ref, *rest):
    kv_in, rest = rest[:n_arr], rest[n_arr:]
    if first:
        state_in = ()
    else:
        state_in, rest = rest[:3], rest[3:]
    if last:
        out_ref, rest = rest[0], rest[1:]
    m_ref, l_ref, acc_ref, kv, ke, qa, qb, s_a, s_b, p_a, p_b, shrink_a, shrink_b, zero_s, todo, sems = rest
    at_keys = 2 if first else 6
    copies = [
        pltpu.make_async_copy(kv_in[n], kv.at[pl.ds(4 * n, 4)], sems.at[n]) for n in range(n_arr)
    ]
    for copy in copies:
        copy.start()
    if first:
        m_ref[...] = jnp.full(m_ref.shape, lowest, jnp.float32)
        l_ref[...] = jnp.zeros(l_ref.shape, jnp.float32)
        acc_ref[...] = jnp.zeros(acc_ref.shape, jnp.float32)
    else:
        m_ref[...] = state_in[0][...]
        l_ref[...] = state_in[1][...]
        acc_ref[...] = state_in[2][...]
    row = lax.broadcasted_iota(jnp.int32, (128, HALF), 0)
    minus_a = jnp.where(row < 3, -1.0, 0.0).astype(jnp.bfloat16)
    minus_b = jnp.where((row >= 3) & (row < 6), -1.0, 0.0).astype(jnp.bfloat16)
    zeros = jnp.zeros((64, HALF), jnp.bfloat16)
    for pq in range(4):
        q = jnp.concatenate([qt_ref[pq, 64 * n : 64 * (n + 1), :] for n in range(4)], axis=1)
        qa[pq, 0:64, :] = q
        qa[pq, 64:128, :] = zeros
        qa[pq, 128:256, :] = minus_a
        qb[pq, 0:64, :] = zeros
        qb[pq, 64:128, :] = q
        qb[pq, 128:256, :] = minus_b
    for copy in copies:
        copy.wait()
    blank = jnp.zeros((112, 128), jnp.float32)

    def prepare(n, carry):
        for k in range(4):
            i = 4 * n + k
            g = kv[i, KROWS + VROWS : KV_ROWS, :].astype(jnp.float32)
            for half in range(2):
                turned = jnp.concatenate([g[16 * half : 16 * (half + 1)], blank], axis=0).T
                ke[i, 128 * half : 128 * (half + 1), :] = turned.astype(jnp.bfloat16)
            zero_s[i] = HALF - jnp.sum(g[8:16]).astype(jnp.int32)
        return carry

    lax.fori_loop(0, n_arr, prepare, 0)

    def list_keys(i, count):
        arr = i // 4
        k_start = ((i % 4) ^ tab[at_keys + 1 + 2 * arr]) * 4096 + tab[at_keys + 2 * arr]
        k_zero = zero_s[i]
        for pq in range(4):
            ahead = (pq ^ tab[1]) * 4096 + tab[0] - k_start
            q_zero = zeros_q[pq]
            live = (ahead > -HALF) & jnp.logical_not((k_zero == HALF) & (q_zero == 0))
            full = (ahead >= HALF) & ((k_zero == 0) | (q_zero == HALF))
            todo[count, 0] = i
            todo[count, 1] = pq
            todo[count, 2] = ahead
            todo[count, 3] = jnp.where(full, 0, 1)
            count = count + live.astype(jnp.int32)
        return count

    count = lax.fori_loop(0, 4 * n_arr, list_keys, 0)
    for extra in range(2):
        todo[count + extra, 0] = 0
        todo[count + extra, 1] = 0
        todo[count + extra, 2] = -100000
        todo[count + extra, 3] = 1

    p_b[...] = jnp.zeros(p_b.shape, jnp.bfloat16)
    shrink_b[...] = jnp.ones(shrink_b.shape, jnp.float32)
    score(todo[0, 0], todo[0, 1], kv, ke, qa, qb, s_a)

    def step(t, now, later):
        s_now, p_now, shrink_now = now
        s_later, p_later, shrink_later = later
        before = jnp.maximum(t - 1, 0)

        @pl.when(todo[t, 3] == 1)
        def _():
            hide(s_now, todo[t, 2], zero_s[todo[t, 0]], zeros_q[todo[t, 1]])

        score(todo[t + 1, 0], todo[t + 1, 1], kv, ke, qa, qb, s_later)
        weigh(todo[t, 1], s_now, p_now, m_ref, l_ref, shrink_now)
        blend(todo[before, 0], todo[before, 1], kv, p_later, shrink_later, acc_ref)

    def two_steps(n, carry):
        side_a, side_b = (s_a, p_a, shrink_a), (s_b, p_b, shrink_b)
        step(2 * n, side_a, side_b)
        step(2 * n + 1, side_b, side_a)
        return carry

    rounds = (count + 1) // 2
    lax.fori_loop(0, rounds, two_steps, 0)

    @pl.when(rounds > 0)
    def _():
        at = 2 * rounds - 1
        blend(todo[at, 0], todo[at, 1], kv, p_b, shrink_b, acc_ref)

    if last:

        def finish(pq, carry):
            out = (acc_ref[pq] / l_ref[pq]).astype(jnp.bfloat16)
            block = pq ^ tab[1]
            for quarter in range(4):
                out_ref[quarter * 4 + block] = out[:, 128 * quarter : 128 * (quarter + 1)]
            return carry

        lax.fori_loop(0, 4, finish, 0)


def attend(table, zeros_q, qt, arrays, state, first, last):
    n_arr = len(arrays)
    vmem = pl.BlockSpec(memory_space=pltpu.VMEM)
    shapes = [
        jax.ShapeDtypeStruct((4, 1, HALF), jnp.float32),
        jax.ShapeDtypeStruct((4, 1, HALF), jnp.float32),
        jax.ShapeDtypeStruct((4, HD, HALF), jnp.float32),
    ]
    scratch = [
        pltpu.VMEM((4 * n_arr, KV_ROWS, 128), jnp.bfloat16),
        pltpu.VMEM((4 * n_arr, 256, 128), jnp.bfloat16),
        pltpu.VMEM((4, 256, HALF), jnp.bfloat16),
        pltpu.VMEM((4, 256, HALF), jnp.bfloat16),
        pltpu.VMEM((2, HALF, 256), jnp.float32),
        pltpu.VMEM((2, HALF, 256), jnp.float32),
        pltpu.VMEM((2, HALF, 256), jnp.bfloat16),
        pltpu.VMEM((2, HALF, 256), jnp.bfloat16),
        pltpu.VMEM((1, HALF), jnp.float32),
        pltpu.VMEM((1, HALF), jnp.float32),
        pltpu.SMEM((4 * n_arr,), jnp.int32),
        pltpu.SMEM((16 * n_arr + 2, 4), jnp.int32),
        pltpu.SemaphoreType.DMA((n_arr,)),
    ]
    if last:
        out_shape = jax.ShapeDtypeStruct((16, HD, 128), jnp.bfloat16)
        out_specs = vmem
        scratch = [pltpu.VMEM(s.shape, s.dtype) for s in shapes] + scratch
    else:
        out_shape = shapes
        out_specs = [vmem] * 3
    state = () if first else tuple(state)
    return pl.pallas_call(
        functools.partial(attend_kernel, n_arr, first, last),
        out_shape=out_shape,
        in_specs=[pl.BlockSpec(memory_space=pltpu.SMEM)] * 2
        + [vmem]
        + [pl.BlockSpec(memory_space=pltpu.HBM)] * n_arr
        + [vmem] * len(state),
        out_specs=out_specs,
        scratch_shapes=scratch,
        compiler_params=pltpu.CompilerParams(vmem_limit_bytes=40 * 1024 * 1024),
        cost_estimate=pl.CostEstimate(
            flops=4_000_000_000 * n_arr, bytes_accessed=1_000_000 * n_arr, transcendentals=0
        ),
        name="attend_first" if first else ("attend_last" if last else "attend_more"),
    )(table, zeros_q, qt, *in_hbm(arrays), *state)


def dense_kernel(sc, att_ref, res_ref, *rest):
    w_in, (mid_ref, gain_ref, w_all, sems) = rest[:8], rest[8:]
    copies = []
    for n in range(8):
        at = pl.multiple_of(sc[18 + n], 128)
        lanes = pl.ds(pl.multiple_of(sc[18 + n] * 2, 256), 256)
        copies.append(pltpu.make_async_copy(w_in[n].at[pl.ds(0, 128)], w_all.at[pl.ds(at, 128)], sems.at[n]))
        copies.append(
            pltpu.make_async_copy(w_in[n].at[pl.ds(128, 8), pl.ds(0, 256)], gain_ref.at[:, lanes], sems.at[8 + n])
        )
    for copy in copies:
        copy.start()
    for copy in copies:
        copy.wait()
    att = att_ref[...].reshape(1024, 128)
    for n in range(8):
        tp = 2 * (n % 4) + n // 4
        cols = slice(256 * tp, 256 * (tp + 1))
        mixed = lax.dot_general(
            att, w_all[:, cols], (((0,), (0,)), ((), ())), preferred_element_type=jnp.float32
        )
        mid_ref[:, cols] = (res_ref[n].astype(jnp.float32) + mixed).astype(jnp.bfloat16)


def dense(scalars, att, res, pieces):
    vmem = pl.BlockSpec(memory_space=pltpu.VMEM)
    return pl.pallas_call(
        dense_kernel,
        out_shape=[
            jax.ShapeDtypeStruct((128, D), jnp.bfloat16),
            jax.ShapeDtypeStruct((8, D), jnp.bfloat16),
        ],
        in_specs=[pl.BlockSpec(memory_space=pltpu.SMEM), vmem, vmem] + [pl.BlockSpec(memory_space=pltpu.HBM)] * 8,
        out_specs=[vmem, vmem],
        scratch_shapes=[pltpu.VMEM((1024, D), jnp.bfloat16), pltpu.SemaphoreType.DMA((16,))],
        compiler_params=pltpu.CompilerParams(vmem_limit_bytes=24 * 1024 * 1024),
        cost_estimate=pl.CostEstimate(flops=1_000_000_000, bytes_accessed=4_000_000, transcendentals=0),
        name="dense",
    )(scalars, att, res, *in_hbm(pieces))


def up_kernel(sc, gain_ref, w_in, *rest):
    mids, (h_ref, own_ref, other_ref, mine_ref, w_up, mid_all, normed, w_down, sems) = rest[:8], rest[8:]
    fetches = [pltpu.make_async_copy(mids[n], mid_all.at[pl.ds(128 * n, 128)], sems.at[16 + n]) for n in range(8)]
    copies = [
        pltpu.make_async_copy(w_in.at[pl.ds(256 * n, 128)], w_up.at[pl.ds(128 * n, 128)], sems.at[n]) for n in range(16)
    ]
    far = []
    for k in range(4):
        at = pl.multiple_of((sc[36 + 2] + k) * 256 + 128, 128)
        far.append(pltpu.make_async_copy(w_in.at[pl.ds(at, 128)], w_down.at[pl.ds(128 * k, 128)], sems.at[24 + k]))
    for copy in fetches + copies + far:
        copy.start()
    gain = gain_ref[0:1, :].astype(jnp.float32)
    lanes = pl.ds(pl.multiple_of(sc[34], 256), 256)
    for n in range(8):
        fetches[n].wait()
        own_ref[pl.ds(pl.multiple_of(sc[26 + n], 128), 128), :] = mid_all[128 * n : 128 * (n + 1), lanes]
        wide = mid_all[128 * n : 128 * (n + 1), :].astype(jnp.float32)
        scale = lax.rsqrt(jnp.sum(wide * wide, axis=-1, keepdims=True) / D + eps)
        normed[128 * n : 128 * (n + 1), :] = (wide * scale * gain).astype(jnp.bfloat16)
    for copy in copies:
        copy.wait()
    for n in range(0, 8, 2):
        h = jnp.dot(normed[128 * n : 128 * (n + 2), :], w_up[...], preferred_element_type=jnp.float32)
        h = jnp.square(jnp.maximum(h, 0.0)).astype(jnp.bfloat16)
        for k in range(2):
            h_ref[pl.ds(pl.multiple_of(sc[26 + n + k], 128), 128), :] = h[128 * k : 128 * (k + 1)]
    for copy in far:
        copy.wait()
    for which, out_ref in ((1 - sc[35], other_ref), (sc[35], mine_ref)):
        rows = w_down[pl.ds(pl.multiple_of(which * 256, 256), 256), :]
        product = lax.dot_general(h_ref[...], rows, (((1,), (1,)), ((), ())), preferred_element_type=jnp.float32)
        out_ref[...] = product.astype(out_ref.dtype)


def up(scalars, gain, w, mids):
    vmem = pl.BlockSpec(memory_space=pltpu.VMEM)
    return pl.pallas_call(
        up_kernel,
        out_shape=[
            jax.ShapeDtypeStruct((1024, 1024), jnp.bfloat16),
            jax.ShapeDtypeStruct((1024, 256), jnp.bfloat16),
            jax.ShapeDtypeStruct((1024, 256), jnp.bfloat16),
            jax.ShapeDtypeStruct((1024, 256), jnp.bfloat16),
        ],
        in_specs=[pl.BlockSpec(memory_space=pltpu.SMEM), vmem] + [pl.BlockSpec(memory_space=pltpu.HBM)] * 9,
        out_specs=[vmem] * 4,
        scratch_shapes=[
            pltpu.VMEM((D, 1024), jnp.bfloat16),
            pltpu.VMEM((1024, D), jnp.bfloat16),
            pltpu.VMEM((1024, D), jnp.bfloat16),
            pltpu.VMEM((512, 1024), jnp.bfloat16),
            pltpu.SemaphoreType.DMA((28,)),
        ],
        compiler_params=pltpu.CompilerParams(vmem_limit_bytes=40 * 1024 * 1024),
        cost_estimate=pl.CostEstimate(flops=5_400_000_000, bytes_accessed=8_000_000, transcendentals=0),
        name="up",
    )(scalars, gain, *in_hbm([w, *mids]))


def down_kernel(steps, sc, h_ref, w_in, *rest):
    count = len(steps)
    outs, (w_down, sems) = rest[: 2 * count], rest[2 * count :]
    copies = []
    for n, r in enumerate(steps):
        for k in range(4):
            at = pl.multiple_of((sc[36 + r] + k) * 256 + 128, 128)
            copies.append(
                pltpu.make_async_copy(
                    w_in.at[pl.ds(at, 128)], w_down.at[pl.ds(128 * (4 * n + k), 128)], sems.at[4 * n + k]
                )
            )
    for copy in copies:
        copy.start()
    for n in range(count):
        for copy in copies[4 * n : 4 * n + 4]:
            copy.wait()
        for which, out_ref in ((1 - sc[35], outs[2 * n]), (sc[35], outs[2 * n + 1])):
            rows = w_down[pl.ds(pl.multiple_of(512 * n + which * 256, 256), 256), :]
            product = lax.dot_general(
                h_ref[...], rows, (((1,), (1,)), ((), ())), preferred_element_type=jnp.float32
            )
            out_ref[...] = product.astype(out_ref.dtype)


def down(scalars, h, w, steps):
    count = len(steps)
    vmem = pl.BlockSpec(memory_space=pltpu.VMEM)
    return pl.pallas_call(
        functools.partial(down_kernel, steps),
        out_shape=[jax.ShapeDtypeStruct((1024, 256), jnp.bfloat16)] * (2 * count),
        in_specs=[pl.BlockSpec(memory_space=pltpu.SMEM), vmem, pl.BlockSpec(memory_space=pltpu.HBM)],
        out_specs=[vmem] * (2 * count),
        scratch_shapes=[pltpu.VMEM((512 * count, 1024), jnp.bfloat16), pltpu.SemaphoreType.DMA((4 * count,))],
        compiler_params=pltpu.CompilerParams(vmem_limit_bytes=24 * 1024 * 1024),
        cost_estimate=pl.CostEstimate(
            flops=1_100_000_000 * count, bytes_accessed=4_000_000, transcendentals=0
        ),
        name="down",
    )(scalars, h, *in_hbm([w]))


def shifted(value, axis, by):
    n = lax.axis_size(axis)
    return lax.ppermute(value, axis, [(i, (i - by) % n) for i in range(n)])


def partner(value):
    return lax.ppermute(value, "c", [(0, 1), (1, 0)])


def places():
    rows = []
    for d in range(128):
        z, y, x, c = d // 32, d // 8 % 4, d // 2 % 4, d % 2
        mask = [(z & 1) | (k << 1) for k in range(2)]
        row = [y * TOK + c * HALF, mask[c]]
        for r in (0,) + RING:
            for half in (c, 1 - c):
                row += [(y + r) % 4 * TOK + half * HALF, mask[half]]
        order = [((x + r) % 4, k) for r in (0,) + RING for k in (c, 1 - c)]
        row += [xs * 256 + k * 128 for xs, k in order]
        row += [k * 512 + xs * 128 for xs, k in order]
        row += [(2 * x + c) * 256, c] + [(x + r) % 4 * 4 for r in range(4)]
        row += [2 * ((z & 1) ^ (k & 1)) + ((z >> 1) ^ (k >> 1)) for k in range(4)]
        rows.append(row)
    return np.asarray(rows, np.int32)


PLACES = places()


def body(queries, keys, values, cum_gates, doc_ids, residual, w_out, norm_gain, w_up, w_down):
    z, y, x, c = (lax.axis_index(a) for a in ("z", "y", "x", "c"))
    table = lax.dynamic_slice(jnp.asarray(PLACES), (((z * 4 + y) * 4 + x) * 2 + c, 0), (1, 44)).reshape(44)

    messages = pack(table, queries, keys, values, jnp.transpose(cum_gates), doc_ids.reshape(1, TOK))

    received = []
    for step in range(4):
        pairs = []
        for zs in range(4):
            for cs in range(2):
                j = 2 * cs + ((zs & 1) ^ (step & 1))
                cd = (zs >> 1) ^ (step >> 1)
                pairs.append((zs * 2 + cs, j * 2 + cd))
        received.append(lax.ppermute(messages[step], ("z", "c"), pairs))
    gain_row = jnp.pad(norm_gain[None], ((0, 7), (0, D - 256)))
    w_msg = jnp.concatenate([w_out, gain_row], axis=0)
    w_mine = [w_msg] + [shifted(w_msg, "x", r) for r in RING]

    qt = jnp.stack([r[KV_ROWS:] for r in received])
    kv_own = jnp.stack([r[:KV_ROWS] for r in received])

    kv_mine = [kv_own] + [shifted(kv_own, "y", r) for r in RING]

    kv_own, residual, w_up, w_down = lax.optimization_barrier((kv_own, residual, w_up, w_down))
    both = jnp.concatenate([w_up, jnp.transpose(w_down)], axis=0)

    docs_own = kv_own[:, KROWS + VROWS + 8 : KROWS + VROWS + 16].astype(jnp.float32)
    zeros_q = (HALF - jnp.sum(docs_own, axis=(1, 2))).astype(jnp.int32)

    kv_near = partner(kv_own)
    state = attend(table, zeros_q, qt, [kv_own, kv_near], (), True, False)
    res = lax.all_to_all(residual.reshape(8, 128, 256), ("c", "x"), 0, 0, tiled=True)
    state, both = lax.optimization_barrier((state, both))
    both = lax.all_gather(both, ("z", "y"), axis=0, tiled=True)
    kv_mine[1:], state = lax.optimization_barrier((kv_mine[1:], state))
    kv_other = [None] + [partner(piece) for piece in kv_mine[1:]]
    pieces = [piece for pair in zip(kv_mine[1:], kv_other[1:]) for piece in pair]
    out = attend(table, zeros_q, qt, pieces, state, False, True)

    w_mine, res, out = lax.optimization_barrier((w_mine, res, out))
    w_pieces = [w for mine in w_mine for w in (mine, partner(mine))]

    attended = lax.all_to_all(out, ("x", "z"), 0, 0, tiled=True)

    middle, gain = dense(table, attended, res, w_pieces)

    mid_mine = [middle] + [shifted(middle, "x", r) for r in RING]
    mids = [m for mine in mid_mine for m in (mine, partner(mine))]
    hidden, middle_own, *far = up(table, gain, both, mids)

    parts = {}
    for name, steps in (("far", (2,)), ("own", (0,)), ("near", (1, 3))):
        if name == "far":
            products = far
        else:
            products = down(table, hidden, both, steps)
        for n, r in enumerate(steps):
            parts[r] = products[2 * n + 1].astype(jnp.float32) + partner(products[2 * n]).astype(jnp.float32)
    total = middle_own.astype(jnp.float32) + parts[0]
    for r in (2, 1, 3):
        total = total + shifted(parts[r].astype(jnp.bfloat16), "x", -r).astype(jnp.float32)
    return total.astype(jnp.bfloat16)


def solution(mesh):
    split = Mesh(mesh.devices.reshape(4, 4, 4, 2), ("z", "y", "x", "c"))
    sp, tp = ("z", "y"), ("x", "c")
    in_specs = (
        P(sp, tp),
        P(sp, tp),
        P(sp, tp),
        P(sp, tp),
        P(sp),
        P(sp, tp),
        P(tp, None),
        P(tp),
        P(sp, tp),
        P(tp, sp),
    )
    return jax.shard_map(body, mesh=split, in_specs=in_specs, out_specs=P(sp, tp), check_vma=False)
```

```python
import functools

import jax
import jax.numpy as jnp
import numpy as np
from jax import lax
from jax.experimental import pallas as pl
from jax.experimental.pallas import tpu as pltpu
from jax.sharding import Mesh, PartitionSpec as P

D = 2048
HD = 64
TOK = 1024
HALF = 512
KROWS = 256
VROWS = 256
GROWS = 32
KV_ROWS = KROWS + VROWS + GROWS
Q_ROWS = 256

eps = 1e-06
far_below = -1e30
lowest = -1e29
RING = (1, 3, 2)


def in_hbm(arrays):
    return [pltpu.with_memory_space_constraint(a, pltpu.HBM) for a in arrays]


def near_in_hbm(arrays):
    return [pltpu.with_memory_space_constraint(a, pltpu.HBM) if n % 2 == 0 else a for n, a in enumerate(arrays)]


def pack_kernel(tab, *rest):
    arrays, outs, (q_ref, v_ref, k_ref, g_ref, d_ref, msgs, sems) = rest[:5], rest[5:9], rest[9:]
    copies = [
        pltpu.make_async_copy(a, to, sems.at[n]) for n, (a, to) in enumerate(zip(arrays, (q_ref, v_ref, k_ref, g_ref, d_ref)))
    ]
    for copy in copies:
        copy.start()
    for copy in copies:
        copy.wait()
    q_t = (q_ref[...].astype(jnp.float32) * 0.125).T.astype(jnp.bfloat16)
    v_t = v_ref[...].astype(jnp.float32).T.astype(jnp.bfloat16)
    docs = d_ref[...].astype(jnp.float32)
    hi = g_ref[...].astype(jnp.bfloat16).astype(jnp.float32)
    rest_of = g_ref[...] - hi
    mid = rest_of.astype(jnp.bfloat16).astype(jnp.float32)
    low = (rest_of - mid).astype(jnp.bfloat16).astype(jnp.float32)

    def blank(rows):
        return jnp.zeros((rows, 128), jnp.float32)

    def chunk(a, row, n):
        return a[row : row + 1, 128 * n : 128 * (n + 1)]

    for head in range(2):
        lanes = slice(64 * head, 64 * (head + 1))
        for half in range(2):
            m = 2 * head + half
            at = HALF * half
            msgs[m, 0:KROWS, :] = jnp.concatenate(
                [k_ref[at : at + 256, lanes], k_ref[at + 256 : at + 512, lanes]], axis=1
            )
            for n in range(4):
                to = KROWS + 64 * n
                msgs[m, to : to + 64, :] = v_t[lanes, at + 128 * n : at + 128 * (n + 1)]
                tokens = at + 128 * n
                to = KV_ROWS + 64 * n
                msgs[m, to : to + 64, :] = q_t[lanes, tokens : tokens + 128]
            for k in range(2):
                rows = [chunk(a, head, 4 * half + k + 2 * side) for side in range(2) for a in (hi, mid, low)]
                rows.append(blank(2))
                if k == 0:
                    rows += [chunk(docs, 0, 4 * half + n) for n in range(4)] + [blank(4)]
                else:
                    rows.append(blank(8))
                to = KROWS + VROWS + 16 * k
                msgs[m, to : to + 16, :] = jnp.concatenate(rows, axis=0).astype(jnp.bfloat16)
    for step in range(4):
        outs[step][...] = msgs[tab[40 + step]]


def pack(table, q, k, v, g, d):
    vmem = pl.BlockSpec(memory_space=pltpu.VMEM)
    rows = KV_ROWS + Q_ROWS
    return pl.pallas_call(
        pack_kernel,
        out_shape=[jax.ShapeDtypeStruct((rows, 128), jnp.bfloat16)] * 4,
        in_specs=[pl.BlockSpec(memory_space=pltpu.SMEM)] + [pl.BlockSpec(memory_space=pltpu.HBM)] * 5,
        out_specs=[vmem] * 4,
        scratch_shapes=[pltpu.VMEM((TOK, 128), jnp.bfloat16)] * 3
        + [
            pltpu.VMEM((2, TOK), jnp.float32),
            pltpu.VMEM((1, TOK), jnp.int32),
            pltpu.VMEM((4, rows, 128), jnp.bfloat16),
            pltpu.SemaphoreType.DMA((5,)),
        ],
        compiler_params=pltpu.CompilerParams(vmem_limit_bytes=16 * 1024 * 1024),
        cost_estimate=pl.CostEstimate(flops=10_000_000, bytes_accessed=2_000_000, transcendentals=0),
        name="pack",
    )(table, *in_hbm([q, v, k, g, d]))


DIMS = (((1,), (0,)), ((), ()))


def score(i, pq, kv, ke, qa, qb, s_ref):
    keys = jnp.concatenate([kv[i, 0:KROWS, :], ke[i]], axis=1)
    for j in range(2):
        for part, q_ref in enumerate((qa, qb)):
            s_ref[j, 256 * part : 256 * (part + 1), :] = lax.dot_general(
                keys, q_ref[pq, :, 256 * j : 256 * (j + 1)], DIMS, preferred_element_type=jnp.float32
            )


def hide(s_ref, ahead, k_zero, q_zero):
    for j in range(2):
        for part in range(2):
            row = lax.broadcasted_iota(jnp.int32, (256, 256), 0)
            lane = lax.broadcasted_iota(jnp.int32, (256, 256), 1)
            seen = (row - lane <= ahead + 256 * (j - part)) & (
                (row >= k_zero - 256 * part) | (lane < q_zero - 256 * j)
            )
            at = slice(256 * part, 256 * (part + 1))
            s_ref[j, at, :] = jnp.where(seen, s_ref[j, at, :], far_below)


def weigh(pq, s_ref, p_ref, m_ref, l_ref, shrink_ref):
    for j in range(2):
        cols = slice(256 * j, 256 * (j + 1))
        top = jnp.max(s_ref[j, 0:64, :].reshape(8, 8, 256), axis=0)
        for n in range(1, 8):
            top = jnp.maximum(top, jnp.max(s_ref[j, 64 * n : 64 * (n + 1), :].reshape(8, 8, 256), axis=0))
        m_old = m_ref[pq, :, cols]
        m_new = jnp.maximum(m_old, jnp.max(top, axis=0, keepdims=True))
        shrink = jnp.exp(m_old - m_new)
        m_ref[pq, :, cols] = m_new
        shrink_ref[:, cols] = shrink
        sums = jnp.zeros((8, 256), jnp.float32)
        for n in range(8):
            p = jnp.exp(s_ref[j, 64 * n : 64 * (n + 1), :] - m_new)
            sums = sums + jnp.sum(p.reshape(8, 8, 256), axis=0)
            p_ref[j, 64 * n : 64 * (n + 1), :] = p.astype(jnp.bfloat16)
        l_ref[pq, :, cols] = l_ref[pq, :, cols] * shrink + jnp.sum(sums, axis=0, keepdims=True)


def blend(i, pq, kv, p_ref, shrink_ref, acc_ref):
    values = jnp.concatenate([kv[i, KROWS + 64 * n : KROWS + 64 * (n + 1), :] for n in range(4)], axis=1)
    for j in range(2):
        cols = slice(256 * j, 256 * (j + 1))
        product = lax.dot_general(values, p_ref[j], DIMS, preferred_element_type=jnp.float32)
        acc_ref[pq, :, cols] = acc_ref[pq, :, cols] * shrink_ref[:, cols] + product


def attend_kernel(n_arr, first, last, tab, zeros_q, qt_ref, *rest):
    kv_in, rest = rest[:n_arr], rest[n_arr:]
    if first:
        state_in = ()
    else:
        state_in, rest = rest[:3], rest[3:]
    if last:
        out_ref, rest = rest[0], rest[1:]
    m_ref, l_ref, acc_ref, kv, ke, qa, qb, s_a, s_b, p_a, p_b, shrink_a, shrink_b, zero_s, todo, sems = rest
    at_keys = 2 if first else 6
    copies = [
        pltpu.make_async_copy(kv_in[n], kv.at[pl.ds(4 * n, 4)], sems.at[n]) for n in range(n_arr)
    ]
    for copy in copies:
        copy.start()
    if first:
        m_ref[...] = jnp.full(m_ref.shape, lowest, jnp.float32)
        l_ref[...] = jnp.zeros(l_ref.shape, jnp.float32)
        acc_ref[...] = jnp.zeros(acc_ref.shape, jnp.float32)
    else:
        m_ref[...] = state_in[0][...]
        l_ref[...] = state_in[1][...]
        acc_ref[...] = state_in[2][...]
    row = lax.broadcasted_iota(jnp.int32, (128, HALF), 0)
    minus_a = jnp.where(row < 3, -1.0, 0.0).astype(jnp.bfloat16)
    minus_b = jnp.where((row >= 3) & (row < 6), -1.0, 0.0).astype(jnp.bfloat16)
    zeros = jnp.zeros((64, HALF), jnp.bfloat16)
    for pq in range(4):
        q = jnp.concatenate([qt_ref[pq, 64 * n : 64 * (n + 1), :] for n in range(4)], axis=1)
        qa[pq, 0:64, :] = q
        qa[pq, 64:128, :] = zeros
        qa[pq, 128:256, :] = minus_a
        qb[pq, 0:64, :] = zeros
        qb[pq, 64:128, :] = q
        qb[pq, 128:256, :] = minus_b
    for copy in copies:
        copy.wait()
    blank = jnp.zeros((112, 128), jnp.float32)

    def prepare(n, carry):
        for k in range(4):
            i = 4 * n + k
            g = kv[i, KROWS + VROWS : KV_ROWS, :].astype(jnp.float32)
            for half in range(2):
                turned = jnp.concatenate([g[16 * half : 16 * (half + 1)], blank], axis=0).T
                ke[i, 128 * half : 128 * (half + 1), :] = turned.astype(jnp.bfloat16)
            zero_s[i] = HALF - jnp.sum(g[8:16]).astype(jnp.int32)
        return carry

    lax.fori_loop(0, n_arr, prepare, 0)

    def list_keys(i, count):
        arr = i // 4
        k_start = ((i % 4) ^ tab[at_keys + 1 + 2 * arr]) * 4096 + tab[at_keys + 2 * arr]
        k_zero = zero_s[i]
        for pq in range(4):
            ahead = (pq ^ tab[1]) * 4096 + tab[0] - k_start
            q_zero = zeros_q[pq]
            live = (ahead > -HALF) & jnp.logical_not((k_zero == HALF) & (q_zero == 0))
            full = (ahead >= HALF) & ((k_zero == 0) | (q_zero == HALF))
            todo[count, 0] = i
            todo[count, 1] = pq
            todo[count, 2] = ahead
            todo[count, 3] = jnp.where(full, 0, 1)
            count = count + live.astype(jnp.int32)
        return count

    count = lax.fori_loop(0, 4 * n_arr, list_keys, 0)
    for extra in range(2):
        todo[count + extra, 0] = 0
        todo[count + extra, 1] = 0
        todo[count + extra, 2] = -100000
        todo[count + extra, 3] = 1

    p_b[...] = jnp.zeros(p_b.shape, jnp.bfloat16)
    shrink_b[...] = jnp.ones(shrink_b.shape, jnp.float32)
    score(todo[0, 0], todo[0, 1], kv, ke, qa, qb, s_a)

    def step(t, now, later):
        s_now, p_now, shrink_now = now
        s_later, p_later, shrink_later = later
        before = jnp.maximum(t - 1, 0)

        @pl.when(todo[t, 3] == 1)
        def _():
            hide(s_now, todo[t, 2], zero_s[todo[t, 0]], zeros_q[todo[t, 1]])

        score(todo[t + 1, 0], todo[t + 1, 1], kv, ke, qa, qb, s_later)
        weigh(todo[t, 1], s_now, p_now, m_ref, l_ref, shrink_now)
        blend(todo[before, 0], todo[before, 1], kv, p_later, shrink_later, acc_ref)

    def two_steps(n, carry):
        side_a, side_b = (s_a, p_a, shrink_a), (s_b, p_b, shrink_b)
        step(2 * n, side_a, side_b)
        step(2 * n + 1, side_b, side_a)
        return carry

    rounds = (count + 1) // 2
    lax.fori_loop(0, rounds, two_steps, 0)

    @pl.when(rounds > 0)
    def _():
        at = 2 * rounds - 1
        blend(todo[at, 0], todo[at, 1], kv, p_b, shrink_b, acc_ref)

    if last:

        def finish(pq, carry):
            out = (acc_ref[pq] / l_ref[pq]).astype(jnp.bfloat16)
            block = pq ^ tab[1]
            for quarter in range(4):
                out_ref[quarter * 4 + block] = out[:, 128 * quarter : 128 * (quarter + 1)]
            return carry

        lax.fori_loop(0, 4, finish, 0)


def attend(table, zeros_q, qt, arrays, state, first, last):
    n_arr = len(arrays)
    vmem = pl.BlockSpec(memory_space=pltpu.VMEM)
    shapes = [
        jax.ShapeDtypeStruct((4, 1, HALF), jnp.float32),
        jax.ShapeDtypeStruct((4, 1, HALF), jnp.float32),
        jax.ShapeDtypeStruct((4, HD, HALF), jnp.float32),
    ]
    scratch = [
        pltpu.VMEM((4 * n_arr, KV_ROWS, 128), jnp.bfloat16),
        pltpu.VMEM((4 * n_arr, 256, 128), jnp.bfloat16),
        pltpu.VMEM((4, 256, HALF), jnp.bfloat16),
        pltpu.VMEM((4, 256, HALF), jnp.bfloat16),
        pltpu.VMEM((2, HALF, 256), jnp.float32),
        pltpu.VMEM((2, HALF, 256), jnp.float32),
        pltpu.VMEM((2, HALF, 256), jnp.bfloat16),
        pltpu.VMEM((2, HALF, 256), jnp.bfloat16),
        pltpu.VMEM((1, HALF), jnp.float32),
        pltpu.VMEM((1, HALF), jnp.float32),
        pltpu.SMEM((4 * n_arr,), jnp.int32),
        pltpu.SMEM((16 * n_arr + 2, 4), jnp.int32),
        pltpu.SemaphoreType.DMA((n_arr,)),
    ]
    if last:
        out_shape = jax.ShapeDtypeStruct((16, HD, 128), jnp.bfloat16)
        out_specs = vmem
        scratch = [pltpu.VMEM(s.shape, s.dtype) for s in shapes] + scratch
    else:
        out_shape = shapes
        out_specs = [vmem] * 3
    state = () if first else tuple(state)
    return pl.pallas_call(
        functools.partial(attend_kernel, n_arr, first, last),
        out_shape=out_shape,
        in_specs=[pl.BlockSpec(memory_space=pltpu.SMEM)] * 2
        + [vmem]
        + [pl.BlockSpec(memory_space=pl.ANY)] * n_arr
        + [vmem] * len(state),
        out_specs=out_specs,
        scratch_shapes=scratch,
        compiler_params=pltpu.CompilerParams(vmem_limit_bytes=40 * 1024 * 1024),
        cost_estimate=pl.CostEstimate(
            flops=4_000_000_000 * n_arr, bytes_accessed=1_000_000 * n_arr, transcendentals=0
        ),
        name="attend_first" if first else ("attend_last" if last else "attend_more"),
    )(table, zeros_q, qt, *near_in_hbm(arrays), *state)


def dense_kernel(sc, att_ref, res_ref, *rest):
    w_in, (mid_ref, gain_ref, w_all, sems) = rest[:8], rest[8:]
    copies = []
    for n in range(8):
        at = pl.multiple_of(sc[18 + n], 128)
        lanes = pl.ds(pl.multiple_of(sc[18 + n] * 2, 256), 256)
        copies.append(pltpu.make_async_copy(w_in[n].at[pl.ds(0, 128)], w_all.at[pl.ds(at, 128)], sems.at[n]))
        copies.append(
            pltpu.make_async_copy(w_in[n].at[pl.ds(128, 8), pl.ds(0, 256)], gain_ref.at[:, lanes], sems.at[8 + n])
        )
    for copy in copies:
        copy.start()
    for copy in copies:
        copy.wait()
    att = att_ref[...].reshape(1024, 128)
    for n in range(8):
        tp = 2 * (n % 4) + n // 4
        cols = slice(256 * tp, 256 * (tp + 1))
        mixed = lax.dot_general(
            att, w_all[:, cols], (((0,), (0,)), ((), ())), preferred_element_type=jnp.float32
        )
        mid_ref[:, cols] = (res_ref[n].astype(jnp.float32) + mixed).astype(jnp.bfloat16)


def dense(scalars, att, res, pieces):
    vmem = pl.BlockSpec(memory_space=pltpu.VMEM)
    return pl.pallas_call(
        dense_kernel,
        out_shape=[
            jax.ShapeDtypeStruct((128, D), jnp.bfloat16),
            jax.ShapeDtypeStruct((8, D), jnp.bfloat16),
        ],
        in_specs=[pl.BlockSpec(memory_space=pltpu.SMEM), vmem, vmem] + [pl.BlockSpec(memory_space=pltpu.HBM)] * 8,
        out_specs=[vmem, vmem],
        scratch_shapes=[pltpu.VMEM((1024, D), jnp.bfloat16), pltpu.SemaphoreType.DMA((16,))],
        compiler_params=pltpu.CompilerParams(vmem_limit_bytes=24 * 1024 * 1024),
        cost_estimate=pl.CostEstimate(flops=1_000_000_000, bytes_accessed=4_000_000, transcendentals=0),
        name="dense",
    )(scalars, att, res, *in_hbm(pieces))


def up_kernel(sc, gain_ref, w_in, *rest):
    mids, (h_ref, own_ref, other_ref, mine_ref, w_up, mid_all, normed, w_down, sems) = rest[:8], rest[8:]
    fetches = [pltpu.make_async_copy(mids[n], mid_all.at[pl.ds(128 * n, 128)], sems.at[16 + n]) for n in range(8)]
    copies = [
        pltpu.make_async_copy(w_in.at[pl.ds(256 * n, 128)], w_up.at[pl.ds(128 * n, 128)], sems.at[n]) for n in range(16)
    ]
    far = []
    for k in range(4):
        at = pl.multiple_of((sc[36 + 2] + k) * 256 + 128, 128)
        far.append(pltpu.make_async_copy(w_in.at[pl.ds(at, 128)], w_down.at[pl.ds(128 * k, 128)], sems.at[24 + k]))
    for copy in fetches + copies + far:
        copy.start()
    gain = gain_ref[0:1, :].astype(jnp.float32)
    lanes = pl.ds(pl.multiple_of(sc[34], 256), 256)
    for n in range(8):
        fetches[n].wait()
        own_ref[pl.ds(pl.multiple_of(sc[26 + n], 128), 128), :] = mid_all[128 * n : 128 * (n + 1), lanes]
        wide = mid_all[128 * n : 128 * (n + 1), :].astype(jnp.float32)
        scale = lax.rsqrt(jnp.sum(wide * wide, axis=-1, keepdims=True) / D + eps)
        normed[128 * n : 128 * (n + 1), :] = (wide * scale * gain).astype(jnp.bfloat16)
    for copy in copies:
        copy.wait()
    for n in range(0, 8, 2):
        h = jnp.dot(normed[128 * n : 128 * (n + 2), :], w_up[...], preferred_element_type=jnp.float32)
        h = jnp.square(jnp.maximum(h, 0.0)).astype(jnp.bfloat16)
        for k in range(2):
            h_ref[pl.ds(pl.multiple_of(sc[26 + n + k], 128), 128), :] = h[128 * k : 128 * (k + 1)]
    for copy in far:
        copy.wait()
    for which, out_ref in ((1 - sc[35], other_ref), (sc[35], mine_ref)):
        rows = w_down[pl.ds(pl.multiple_of(which * 256, 256), 256), :]
        product = lax.dot_general(h_ref[...], rows, (((1,), (1,)), ((), ())), preferred_element_type=jnp.float32)
        out_ref[...] = product.astype(out_ref.dtype)


def up(scalars, gain, w, mids):
    vmem = pl.BlockSpec(memory_space=pltpu.VMEM)
    return pl.pallas_call(
        up_kernel,
        out_shape=[
            jax.ShapeDtypeStruct((1024, 1024), jnp.bfloat16),
            jax.ShapeDtypeStruct((1024, 256), jnp.bfloat16),
            jax.ShapeDtypeStruct((1024, 256), jnp.bfloat16),
            jax.ShapeDtypeStruct((1024, 256), jnp.bfloat16),
        ],
        in_specs=[pl.BlockSpec(memory_space=pltpu.SMEM), vmem] + [pl.BlockSpec(memory_space=pl.ANY)] * 9,
        out_specs=[vmem] * 4,
        scratch_shapes=[
            pltpu.VMEM((D, 1024), jnp.bfloat16),
            pltpu.VMEM((1024, D), jnp.bfloat16),
            pltpu.VMEM((1024, D), jnp.bfloat16),
            pltpu.VMEM((512, 1024), jnp.bfloat16),
            pltpu.SemaphoreType.DMA((28,)),
        ],
        compiler_params=pltpu.CompilerParams(vmem_limit_bytes=40 * 1024 * 1024),
        cost_estimate=pl.CostEstimate(flops=5_400_000_000, bytes_accessed=8_000_000, transcendentals=0),
        name="up",
    )(scalars, gain, *in_hbm([w]), *near_in_hbm(mids))


def down_kernel(steps, sc, h_ref, w_in, *rest):
    count = len(steps)
    outs, (w_down, sems) = rest[: 2 * count], rest[2 * count :]
    copies = []
    for n, r in enumerate(steps):
        for k in range(4):
            at = pl.multiple_of((sc[36 + r] + k) * 256 + 128, 128)
            copies.append(
                pltpu.make_async_copy(
                    w_in.at[pl.ds(at, 128)], w_down.at[pl.ds(128 * (4 * n + k), 128)], sems.at[4 * n + k]
                )
            )
    for copy in copies:
        copy.start()
    for n in range(count):
        for copy in copies[4 * n : 4 * n + 4]:
            copy.wait()
        for which, out_ref in ((1 - sc[35], outs[2 * n]), (sc[35], outs[2 * n + 1])):
            rows = w_down[pl.ds(pl.multiple_of(512 * n + which * 256, 256), 256), :]
            product = lax.dot_general(
                h_ref[...], rows, (((1,), (1,)), ((), ())), preferred_element_type=jnp.float32
            )
            out_ref[...] = product.astype(out_ref.dtype)


def down(scalars, h, w, steps):
    count = len(steps)
    vmem = pl.BlockSpec(memory_space=pltpu.VMEM)
    return pl.pallas_call(
        functools.partial(down_kernel, steps),
        out_shape=[jax.ShapeDtypeStruct((1024, 256), jnp.bfloat16)] * (2 * count),
        in_specs=[pl.BlockSpec(memory_space=pltpu.SMEM), vmem, pl.BlockSpec(memory_space=pltpu.HBM)],
        out_specs=[vmem] * (2 * count),
        scratch_shapes=[pltpu.VMEM((512 * count, 1024), jnp.bfloat16), pltpu.SemaphoreType.DMA((4 * count,))],
        compiler_params=pltpu.CompilerParams(vmem_limit_bytes=24 * 1024 * 1024),
        cost_estimate=pl.CostEstimate(
            flops=1_100_000_000 * count, bytes_accessed=4_000_000, transcendentals=0
        ),
        name="down",
    )(scalars, h, *in_hbm([w]))


def shifted(value, axis, by):
    n = lax.axis_size(axis)
    return lax.ppermute(value, axis, [(i, (i - by) % n) for i in range(n)])


def partner(value):
    return lax.ppermute(value, "c", [(0, 1), (1, 0)])


def places():
    rows = []
    for d in range(128):
        z, y, x, c = d // 32, d // 8 % 4, d // 2 % 4, d % 2
        mask = [(z & 1) | (k << 1) for k in range(2)]
        row = [y * TOK + c * HALF, mask[c]]
        for r in (0,) + RING:
            for half in (c, 1 - c):
                row += [(y + r) % 4 * TOK + half * HALF, mask[half]]
        order = [((x + r) % 4, k) for r in (0,) + RING for k in (c, 1 - c)]
        row += [xs * 256 + k * 128 for xs, k in order]
        row += [k * 512 + xs * 128 for xs, k in order]
        row += [(2 * x + c) * 256, c] + [(x + r) % 4 * 4 for r in range(4)]
        row += [2 * ((z & 1) ^ (k & 1)) + ((z >> 1) ^ (k >> 1)) for k in range(4)]
        rows.append(row)
    return np.asarray(rows, np.int32)


PLACES = places()


def body(queries, keys, values, cum_gates, doc_ids, residual, w_out, norm_gain, w_up, w_down):
    z, y, x, c = (lax.axis_index(a) for a in ("z", "y", "x", "c"))
    table = lax.dynamic_slice(jnp.asarray(PLACES), (((z * 4 + y) * 4 + x) * 2 + c, 0), (1, 44)).reshape(44)

    messages = pack(table, queries, keys, values, jnp.transpose(cum_gates), doc_ids.reshape(1, TOK))

    received = []
    for step in range(4):
        pairs = []
        for zs in range(4):
            for cs in range(2):
                j = 2 * cs + ((zs & 1) ^ (step & 1))
                cd = (zs >> 1) ^ (step >> 1)
                pairs.append((zs * 2 + cs, j * 2 + cd))
        received.append(lax.ppermute(messages[step], ("z", "c"), pairs))
    gain_row = jnp.pad(norm_gain[None], ((0, 7), (0, D - 256)))
    w_msg = jnp.concatenate([w_out, gain_row], axis=0)
    w_mine = [w_msg] + [shifted(w_msg, "x", r) for r in RING]

    qt = jnp.stack([r[KV_ROWS:] for r in received])
    kv_own = jnp.stack([r[:KV_ROWS] for r in received])

    kv_mine = [kv_own] + [shifted(kv_own, "y", r) for r in RING]

    kv_own, residual, w_up, w_down = lax.optimization_barrier((kv_own, residual, w_up, w_down))
    both = jnp.concatenate([w_up, jnp.transpose(w_down)], axis=0)

    docs_own = kv_own[:, KROWS + VROWS + 8 : KROWS + VROWS + 16].astype(jnp.float32)
    zeros_q = (HALF - jnp.sum(docs_own, axis=(1, 2))).astype(jnp.int32)

    kv_near = partner(kv_own)
    state = attend(table, zeros_q, qt, [kv_own, kv_near], (), True, False)
    res = lax.all_to_all(residual.reshape(8, 128, 256), ("c", "x"), 0, 0, tiled=True)
    state, both = lax.optimization_barrier((state, both))
    both = lax.all_gather(both, ("z", "y"), axis=0, tiled=True)
    kv_mine[1:], state = lax.optimization_barrier((kv_mine[1:], state))
    kv_other = [None] + [partner(piece) for piece in kv_mine[1:]]
    pieces = [piece for pair in zip(kv_mine[1:], kv_other[1:]) for piece in pair]
    out = attend(table, zeros_q, qt, pieces, state, False, True)

    w_mine, res, out = lax.optimization_barrier((w_mine, res, out))
    w_pieces = [w for mine in w_mine for w in (mine, partner(mine))]

    attended = lax.all_to_all(out, ("x", "z"), 0, 0, tiled=True)

    middle, gain = dense(table, attended, res, w_pieces)

    mid_mine = [middle] + [shifted(middle, "x", r) for r in RING]
    mids = [m for mine in mid_mine for m in (mine, partner(mine))]
    hidden, middle_own, *far = up(table, gain, both, mids)

    parts = {}
    for name, steps in (("far", (2,)), ("own", (0,)), ("near", (1, 3))):
        if name == "far":
            products = far
        else:
            products = down(table, hidden, both, steps)
        for n, r in enumerate(steps):
            parts[r] = products[2 * n + 1].astype(jnp.float32) + partner(products[2 * n]).astype(jnp.float32)
    total = middle_own.astype(jnp.float32) + parts[0]
    for r in (2, 1, 3):
        total = total + shifted(parts[r].astype(jnp.bfloat16), "x", -r).astype(jnp.float32)
    return total.astype(jnp.bfloat16)


def solution(mesh):
    split = Mesh(mesh.devices.reshape(4, 4, 4, 2), ("z", "y", "x", "c"))
    sp, tp = ("z", "y"), ("x", "c")
    in_specs = (
        P(sp, tp),
        P(sp, tp),
        P(sp, tp),
        P(sp, tp),
        P(sp),
        P(sp, tp),
        P(tp, None),
        P(tp),
        P(sp, tp),
        P(tp, sp),
    )
    return jax.shard_map(body, mesh=split, in_specs=in_specs, out_specs=P(sp, tp), check_vma=False)
```
